256 devices in a mesh: sp: 16 (over y, x), dp: 16 (over z, core).
Axes of the slice: x: 4, y: 4, z: 8, core: 2. Of those that a mesh axis runs over, the one named last changes fastest.
Arguments:
- tokens: bfloat16 [16, 4096, 2048], P('dp', 'sp'), may hold values from -6 to 6
- in_gain: float32 [2048], replicated, may hold values from 0.1 to 1.9
- query_weight: bfloat16 [2048, 2048], P('dp'), may hold values from -1 to 1
- key_weight: bfloat16 [2048, 512], P('dp'), may hold values from -1 to 1
- value_matrix: bfloat16 [2048, 512], P('dp'), may hold values from -0.125 to 0.125
- query_gain: float32 [128], replicated, may hold values from 1 to 6
- key_gain: float32 [128], replicated, may hold values from 1 to 6
- out_weight: bfloat16 [2048, 2048], P('dp'), may hold values from -0.125 to 0.125
- out_gain: float32 [2048], replicated, may hold values from 0.1 to 1.9
Outputs:
- mixed: bfloat16 [16, 4096, 2048], P('dp', 'sp')
The draws below stay inside these ranges and needn't reach their ends.
All inputs are finite; a program needn't handle non-finite values.
Results may differ from the reference program's by a relative error of at most 0.0055.
The reference program's roundings to bfloat16 on the way count: a program that leaves them out, or rounds other values in their place, can miss the bound.
Values may be sent and summed in bfloat16 or wider, within the bound.
A program may use at most 128 MiB of HBM per device.

```python
import jax
import jax.numpy as jnp
from jax import lax

MODEL_WIDTH = 2048
QUERY_HEAD_COUNT = 16
KEY_VALUE_HEADS = 4
HEAD_WIDTH = 128
GRID_W = 64
SEQUENCE_LENGTH = 4096
BATCH = 16


def query_for_group(key):
    return jax.random.truncated_normal(jax.random.fold_in(key, 101), -6.0, 6.0, (MODEL_WIDTH, QUERY_HEAD_COUNT * HEAD_WIDTH), jnp.float32) * MODEL_WIDTH ** (-0.5)


def draw_query_weight(key, part):
    return query_for_group(key).astype(jnp.bfloat16)


def draw_key_weight(key, part):
    complete_output = jax.random.truncated_normal(jax.random.fold_in(key, 401), -6.0, 6.0, (MODEL_WIDTH, KEY_VALUE_HEADS * HEAD_WIDTH), jnp.float32) * MODEL_WIDTH ** (-0.5)
    return complete_output.astype(jnp.bfloat16)


def draw_query_gain(key, part):
    return 1.6 * (1.0 + 0.18 * jax.random.uniform(jax.random.fold_in(key, 201), (HEAD_WIDTH,), jnp.float32, -1.0, 1.0))


def draw_key_gain(key, part):
    return 1.6 * (1.0 + 0.18 * jax.random.uniform(jax.random.fold_in(key, 301), (HEAD_WIDTH,), jnp.float32, -1.0, 1.0))


def level_of(key, dims, split, low, largest):
    def one(dim, shards_of):
        heights = jax.random.uniform(jax.random.fold_in(jax.random.fold_in(key, 6), dim), (shards_of,), jnp.float32, low / len(split), largest / len(split))
        return jnp.repeat(jnp.exp(heights), dims[dim] // shards_of).reshape((-1,) + (1,) * (len(dims) - dim - 1))

    level = one(*split[0])
    for cut in split[1:]:
        level = level * one(*cut)
    return level


def gaussian(rng, extent, deviation, reach, pieces=(), kind=jnp.bfloat16):
    drawn = deviation * jax.random.normal(rng, extent, jnp.float32)
    if pieces:
        drawn = drawn * level_of(rng, extent, pieces, -0.22, 0.18)
    return jnp.clip(drawn, -reach, reach).astype(kind)


def setup_inputs(seed: int = 0) -> dict:
    seeds = jax.random.split(jax.random.key(seed), 10)
    return {
        "tokens": gaussian(seeds[0], (BATCH, SEQUENCE_LENGTH, MODEL_WIDTH), 1.0, 6.0, ((0, 16), (1, 16))),
        "in_gain": jnp.clip(1.0 + 0.18 * jax.random.normal(seeds[1], (MODEL_WIDTH,), jnp.float32), 0.1, 1.9),
        "query_weight": draw_query_weight(jax.random.fold_in(seeds[9], 71), 0),
        "key_weight": draw_key_weight(jax.random.fold_in(seeds[9], 71), 0),
        "value_matrix": gaussian(seeds[4], (MODEL_WIDTH, KEY_VALUE_HEADS * HEAD_WIDTH), MODEL_WIDTH ** -0.5, 0.125, ((0, 16),)),
        "query_gain": draw_query_gain(jax.random.fold_in(seeds[9], 71), 0),
        "key_gain": draw_key_gain(jax.random.fold_in(seeds[9], 71), 0),
        "out_weight": gaussian(seeds[7], (QUERY_HEAD_COUNT * HEAD_WIDTH, MODEL_WIDTH), (QUERY_HEAD_COUNT * HEAD_WIDTH) ** -0.5, 0.125, ((0, 16),)),
        "out_gain": jnp.clip(1.0 + 0.18 * jax.random.normal(seeds[8], (MODEL_WIDTH,), jnp.float32), 0.1, 1.9),
    }


EPS = 1e-06
THETA = 10000.0

def norm_rows(row_data, gain_vec):
    return row_data * lax.rsqrt(lax.optimization_barrier(jnp.mean(row_data * row_data, axis=-1, keepdims=True)) + EPS) * gain_vec.astype(jnp.float32)

def rotate(head_data, positions):
    head_size = head_data.shape[-1]
    half_size = head_size // 2
    quarter = head_size // 4
    inverse_freq = THETA ** (-jnp.arange(quarter, dtype=jnp.float32) / quarter)
    row_angle = (positions // GRID_W).astype(jnp.float32)[:, None] * inverse_freq[None, :]
    col_angle = (positions % GRID_W).astype(jnp.float32)[:, None] * inverse_freq[None, :]

    def turn_half(half_part, angle):
        cosine = jnp.cos(angle)[:, None, :]
        sine_val = jnp.sin(angle)[:, None, :]
        first_part = half_part[..., :quarter]
        second_part = half_part[..., quarter:]
        return jnp.concatenate([first_part * cosine - second_part * sine_val, second_part * cosine + first_part * sine_val], axis=-1)
    return jnp.concatenate([turn_half(head_data[..., :half_size], row_angle), turn_half(head_data[..., half_size:], col_angle)], axis=-1)

def finish(projected, gain_vec, positions):
    row_count = projected.shape[0]
    heads_data = projected.reshape(row_count, -1, HEAD_WIDTH)
    heads_data = rotate(norm_rows(heads_data, gain_vec), positions)
    return heads_data.reshape(row_count, -1).astype(jnp.bfloat16)

def reference(tokens, in_gain, query_weight, key_weight, value_matrix, query_gain, key_gain, out_weight, out_gain):
    queries_per_group = QUERY_HEAD_COUNT // KEY_VALUE_HEADS
    rows_per_block = min(512, SEQUENCE_LENGTH)

    def per_sequence(sequence):
        float_rows = sequence.astype(jnp.float32)
        normed = norm_rows(float_rows, in_gain).astype(jnp.bfloat16)
        positions = jnp.arange(SEQUENCE_LENGTH, dtype=jnp.int32)
        query_rows = finish(jnp.dot(normed, query_weight, preferred_element_type=jnp.float32), query_gain, positions)
        key_matrix_rows = finish(jnp.dot(normed, key_weight, preferred_element_type=jnp.float32), key_gain, positions)
        value_rows = jnp.dot(normed, value_matrix, preferred_element_type=jnp.float32).astype(jnp.bfloat16)
        key_rows_float = key_matrix_rows.reshape(SEQUENCE_LENGTH, KEY_VALUE_HEADS, HEAD_WIDTH).astype(jnp.float32)
        value_rows_float = value_rows.reshape(SEQUENCE_LENGTH, KEY_VALUE_HEADS, HEAD_WIDTH).astype(jnp.float32)
        query_block_list = query_rows.reshape(SEQUENCE_LENGTH // rows_per_block, rows_per_block, KEY_VALUE_HEADS, queries_per_group, HEAD_WIDTH)

        def attend(query_block):
            scores = jnp.einsum('qegd,ked->egqk', query_block.astype(jnp.float32), key_rows_float) * HEAD_WIDTH ** (-0.5)
            shifted = scores - lax.optimization_barrier(jnp.max(scores, axis=-1, keepdims=True))
            raised = jnp.exp(shifted)
            weights = (raised / lax.optimization_barrier(jnp.sum(raised, axis=-1, keepdims=True))).astype(jnp.bfloat16)
            attended = jnp.einsum('egqk,ked->qegd', weights.astype(jnp.float32), value_rows_float)
            return attended.astype(jnp.bfloat16)
        attended = lax.map(attend, query_block_list).reshape(SEQUENCE_LENGTH, QUERY_HEAD_COUNT * HEAD_WIDTH)
        projected = jnp.dot(attended, out_weight, preferred_element_type=jnp.float32)
        return norm_rows(projected, out_gain).astype(jnp.bfloat16)
    return lax.map(per_sequence, tokens)
```

```python
import jax
import jax.numpy as jnp
from jax import lax
from jax.experimental import pallas as pl
from jax.experimental.pallas import tpu as pltpu
from jax.sharding import PartitionSpec as P

MESH = pl.DeviceIdType.MESH
F32 = jnp.float32
BF16 = jnp.bfloat16

EPS = 1e-06
THETA = 10000.0
GRID_W = 64
HEAD = 128
WIDTH = 2048
ROWS = 256
GROUP = 4
KEYS = GROUP * ROWS
Z = 8
SHARD = WIDTH // (2 * Z)
CUT = 768
HALF = ROWS // 2
BQ = 512
TILES = KEYS * GROUP // BQ
ONES = 16
LOG2E = 1.4426950408889634


def span(index, size):
    return pl.ds(pl.multiple_of(index * size, size), size)


def kernel(
    tokens,
    in_gain,
    wq,
    wk,
    wv,
    q_gain,
    k_gain,
    wo,
    out_gain,
    out,
    raw,
    normed,
    weights,
    out_weights,
    cosines,
    sines,
    qt,
    kbuf,
    vbuf,
    s0,
    s1,
    top0,
    top1,
    row_max,
    acc,
    attended,
    returned,
    projected,
    ag_send,
    ag_recv,
    zw_send,
    zw_recv,
    cw_send,
    cw_recv,
    zo_send,
    zo_recv,
    co_send,
    co_recv,
    kv_send,
    kv_recv,
    ret_send,
    ret_recv,
):
    sp = lax.axis_index("sp")
    dp = lax.axis_index("dp")
    y, x = sp // 4, sp % 4
    z, core = dp // 2, dp % 2
    at = (1 - core) * y + core * x
    group = (y + x) % 4

    def member(step):
        to = (at + step) % 4
        return (1 - core) * (to * 4 + x) + core * (y * 4 + to)

    def diagonal(step):
        return ((y + 4 - step) % 4) * 4 + (x + step) % 4

    up = {"dp": ((z + 1) % Z) * 2 + core}
    down = {"dp": ((z + Z - 1) % Z) * 2 + core}
    twin = {"dp": z * 2 + 1 - core}
    peers = [{"sp": member(1)}, {"sp": member(3)}, {"sp": member(2)}]
    peers += [{"sp": diagonal(1)}, {"sp": diagonal(3)}, up, down, twin]

    barrier = pltpu.get_barrier_semaphore()
    for peer in peers:
        pl.semaphore_signal(barrier, inc=1, device_id=peer, device_id_type=MESH)
    pl.semaphore_wait(barrier, len(peers))

    sent = []

    def send(src, dst, send_sem, recv_sem, to):
        copy = pltpu.make_async_remote_copy(
            src_ref=src,
            dst_ref=dst,
            send_sem=send_sem,
            recv_sem=recv_sem,
            device_id=to,
            device_id_type=MESH,
        )
        copy.start()
        return copy

    def arrival(ref, sem):
        pltpu.make_async_copy(ref, ref, sem).wait()

    low, high = pl.ds(0, HALF), pl.ds(HALF, HALF)
    nxt, prv = {"sp": member(1)}, {"sp": member(3)}

    def token_send(src, slot, part, index, to):
        sent.append(
            send(src, raw.at[slot - 1, part], ag_send.at[index], ag_recv.at[index], to)
        )

    token_send(tokens.at[0, low], 3, low, 0, nxt)
    token_send(tokens.at[0, high], 1, high, 1, prv)
    token_send(tokens.at[0, high], 3, high, 2, nxt)
    token_send(tokens.at[0, low], 1, low, 3, prv)

    chunks = (pl.ds(0, SHARD // 2), pl.ds(SHARD // 2, SHARD // 2))
    q_cols = span(group, 512)
    kv_cols = span(group, HEAD)

    def first_weights(part, send_sem, recv_sem, to):
        mine = weights.at[dp, part]
        for src, cols in (
            (wq.at[part, q_cols], pl.ds(0, 512)),
            (wk.at[part, kv_cols], pl.ds(512, HEAD)),
            (wv.at[part, kv_cols], pl.ds(640, HEAD)),
        ):
            send(src, mine.at[:, cols], send_sem, recv_sem, to)
        sent.append(
            pltpu.make_async_remote_copy(
                src_ref=mine,
                dst_ref=mine,
                send_sem=send_sem,
                recv_sem=recv_sem,
                device_id=to,
                device_id_type=MESH,
            )
        )

    for i in (0, 1):
        first_weights(chunks[i], zw_send.at[0, 0, i], zw_recv.at[0, 0, i], up)
        first_weights(chunks[i], zw_send.at[1, 0, i], zw_recv.at[1, 0, i], down)
    for i in (0, 1):
        first_weights(chunks[i], cw_send.at[0, i], cw_recv.at[0, i], twin)

    weights[dp, :, 0:512] = wq[:, q_cols]
    weights[dp, :, 512:640] = wk[:, kv_cols]
    weights[dp, :, 640:768] = wv[:, kv_cols]
    out_weights[dp] = wo[...]

    def ring_event(buf, zs, zr, cs, cr, way, step, i):
        source = (((z + Z - step) % Z) if way == 0 else ((z + step) % Z)) * 2 + core
        part = buf.at[source, chunks[i]]
        arrival(part, zr.at[way, step - 1, i])
        if step < 3 or (step == 3 and i == way):
            sent.append(
                send(part, part, zs.at[way, step, i], zr.at[way, step, i], (up, down)[way])
            )
        slot = step if way == 0 else Z - step
        sent.append(send(part, part, cs.at[slot, i], cr.at[slot, i], twin))

    def weight_event(way, step, i):
        ring_event(weights, zw_send, zw_recv, cw_send, cw_recv, way, step, i)

    def out_event(way, step, i):
        ring_event(out_weights, zo_send, zo_recv, co_send, co_recv, way, step, i)

    gain_in = in_gain[...]

    def normalize(src, slot):
        def rows(i, c):
            part = pl.ds(pl.multiple_of(i * 32, 32), 32)
            v = src[part, :].astype(F32)
            ms = jnp.mean(v * v, axis=-1, keepdims=True)
            normed[slot, part, :] = (v * lax.rsqrt(ms + EPS) * gain_in).astype(BF16)
            return c

        lax.fori_loop(0, ROWS // 32, rows, 0)

    def angles(slot, c):
        row = lax.broadcasted_iota(jnp.int32, (ROWS, HEAD), 0)
        lane = lax.broadcasted_iota(jnp.int32, (ROWS, HEAD), 1)
        power = (lane % 32).astype(F32) * (1.0 / 32.0)
        freq = jnp.exp(power * (-9.210340371976184))
        grid_row = member(slot) * (ROWS // GRID_W) + row // GRID_W
        place = jnp.where(lane < 64, grid_row, row % GRID_W).astype(F32)
        angle = place * freq
        cosines[slot] = jnp.cos(angle)
        sine = jnp.sin(angle)
        sines[slot] = jnp.where(lane % 64 < 32, -sine, sine)
        return c

    for i in (0, 1):
        weight_event(0, 1, i)
        weight_event(1, 1, i)
    normalize(tokens.at[0], 0)
    arrival(raw.at[2, low], ag_recv.at[0])
    token_send(raw.at[2, low], 2, low, 4, nxt)
    arrival(raw.at[0, high], ag_recv.at[1])
    token_send(raw.at[0, high], 2, high, 5, prv)
    for i in (0, 1):
        weight_event(0, 2, i)
        weight_event(1, 2, i)
    lax.fori_loop(0, GROUP, angles, 0)
    for i in (0, 1):
        weight_event(0, 3, i)
        weight_event(1, 3, i)
    arrival(raw.at[2, high], ag_recv.at[2])
    arrival(raw.at[0, low], ag_recv.at[3])
    normalize(raw.at[2], 3)
    normalize(raw.at[0], 1)
    weight_event(0, 4, 0)
    weight_event(1, 4, 1)

    for i in (0, 1):
        for way, to in ((0, up), (1, down)):
            part = out_weights.at[dp, chunks[i]]
            sent.append(
                send(wo.at[chunks[i]], part, zo_send.at[way, 0, i], zo_recv.at[way, 0, i], to)
            )
    for i in (0, 1):
        part = out_weights.at[dp, chunks[i]]
        sent.append(send(wo.at[chunks[i]], part, co_send.at[0, i], co_recv.at[0, i], twin))

    def twin_arrivals(buf, cr):
        for slot in range(Z):
            source = ((z + Z - slot) % Z) * 2 + 1 - core
            for i in (0, 1):
                arrival(buf.at[source, chunks[i]], cr.at[slot, i])

    twin_arrivals(weights, cw_recv)
    arrival(raw.at[1, low], ag_recv.at[4])
    arrival(raw.at[1, high], ag_recv.at[5])
    normalize(raw.at[1], 2)

    gain_q, gain_k = q_gain[...], k_gain[...]

    def project(slot, c):
        cut = weights[...].reshape(WIDTH, CUT)
        values = jnp.dot(normed[slot], cut, preferred_element_type=F32)
        cosine, sine = cosines[slot], sines[slot]
        lane = lax.broadcasted_iota(jnp.int32, (ROWS, HEAD), 1)
        first = lane % 64 < 32

        def finish(v, gain):
            ms = jnp.mean(v * v, axis=-1, keepdims=True)
            v = v * lax.rsqrt(ms + EPS) * gain
            other = jnp.where(first, pltpu.roll(v, HEAD - 32, 1), pltpu.roll(v, 32, 1))
            return v * cosine + other * sine

        for h in range(4):
            q = finish(values[:, h * HEAD : (h + 1) * HEAD], gain_q)
            q = q.astype(BF16).astype(F32).T * (HEAD**-0.5 * LOG2E)
            coarse = q.astype(BF16)
            fine = (q - coarse.astype(F32)).astype(BF16)
            cols = pl.ds(pl.multiple_of(slot * KEYS + h * ROWS, ROWS), ROWS)
            qt[0:HEAD, cols] = coarse
            qt[HEAD : 2 * HEAD, cols] = fine
        rows = span(slot, ROWS)
        kbuf[0, rows, :] = finish(values[:, 512:640], gain_k).astype(BF16)
        vbuf[0, 0:HEAD, rows] = values[:, 640:768].T.astype(BF16)
        return c

    lax.fori_loop(0, GROUP, project, 0)

    def kv_send_to(src, slot, what, index, to):
        buf = kbuf if what == 0 else vbuf
        whole = pl.ds(0, KEYS) if what == 0 else pl.ds(0, HEAD)
        sent.append(
            send(
                buf.at[src, whole],
                buf.at[slot, whole],
                kv_send.at[index],
                kv_recv.at[index],
                {"sp": diagonal(to)},
            )
        )

    kv_send_to(0, 3, 0, 0, 1)
    kv_send_to(0, 1, 1, 1, 3)
    kv_send_to(0, 3, 1, 2, 1)
    kv_send_to(0, 1, 0, 3, 3)

    ones = jnp.ones((ONES, KEYS), BF16)
    for d in range(GROUP):
        vbuf[d, HEAD : HEAD + ONES, :] = ones
    row_max[...] = jnp.full_like(row_max, -1e30)
    acc[...] = jnp.zeros_like(acc)

    def attend(block, nt, sn, topn, ct, sc, topc):
        size = 256
        if sc is not None:
            cols = span(ct, BQ)
            old = row_max[:, cols]
            new = jnp.maximum(old, jnp.max(topc[...], axis=0, keepdims=True))
            row_max[:, cols] = new
            decay = jnp.exp2(old - new)
        top, total = None, None
        for c in range(KEYS // size):
            part = pl.ds(c * size, size)
            if sn is not None:
                k = kbuf[block, part, :]
                s = jnp.dot(
                    jnp.concatenate([k, k], axis=1),
                    qt[:, span(nt, BQ)],
                    preferred_element_type=F32,
                )
                sn[part, :] = s
                most = jnp.max(s.reshape(size // 8, 8, BQ), axis=0)
                top = most if top is None else jnp.maximum(top, most)
            if sc is not None:
                p = jnp.exp2(sc[part, :] - new).astype(BF16)
                d = jnp.dot(vbuf[block, :, part], p, preferred_element_type=F32)
                total = d if total is None else total + d
        if sn is not None:
            topn[...] = top
        if sc is not None:
            acc[:, cols] = acc[:, cols] * decay + total

    def attend_block(block):
        attend(block, 0, s0, top0, None, None, None)

        def pair(i, c):
            t = i * 2
            attend(block, t + 1, s1, top1, t, s0, top0)
            attend(block, (t + 2) % TILES, s0, top0, t + 1, s1, top1)
            return c

        lax.fori_loop(0, TILES // 2, pair, 0)

    attend_block(0)
    for i in (0, 1):
        out_event(0, 1, i)
        out_event(1, 1, i)
    k_all, v_all = pl.ds(0, KEYS), pl.ds(0, HEAD)
    arrival(kbuf.at[3, k_all], kv_recv.at[0])
    kv_send_to(3, 2, 0, 4, 1)
    arrival(vbuf.at[1, v_all], kv_recv.at[1])
    kv_send_to(1, 2, 1, 5, 3)
    arrival(vbuf.at[3, v_all], kv_recv.at[2])
    arrival(kbuf.at[1, k_all], kv_recv.at[3])
    attend_block(3)
    attend_block(1)
    for i in (0, 1):
        out_event(0, 2, i)
        out_event(1, 2, i)
    arrival(kbuf.at[2, k_all], kv_recv.at[4])
    arrival(vbuf.at[2, v_all], kv_recv.at[5])
    attend_block(2)

    def hand_back(slot):
        for h in range(4):
            cols = pl.ds(slot * KEYS + h * ROWS, ROWS)
            scaled = acc[0:HEAD, cols] / acc[HEAD : HEAD + 1, cols]
            attended[slot, :, h * HEAD : (h + 1) * HEAD] = scaled.T.astype(BF16)

    for slot in (2, 1, 3):
        hand_back(slot)
        sent.append(
            send(
                attended.at[slot],
                returned.at[group],
                ret_send.at[slot - 1],
                ret_recv.at[slot - 1],
                {"sp": member(slot)},
            )
        )
    hand_back(0)
    returned[group] = attended[0]
    for i in (0, 1):
        out_event(0, 3, i)
        out_event(1, 3, i)
    out_event(0, 4, 0)
    out_event(1, 4, 1)
    for slot in (1, 2, 3):
        arrival(returned.at[(group + 4 - slot) % 4], ret_recv.at[slot - 1])
    twin_arrivals(out_weights, co_recv)

    squares = jnp.zeros((ROWS, 1), F32)
    for n in range(4):
        cols = slice(n * 512, (n + 1) * 512)
        total = None
        for g in range(4):
            w = out_weights[g * 4 : (g + 1) * 4, :, cols].reshape(512, 512)
            d = jnp.dot(returned[g], w, preferred_element_type=F32)
            total = d if total is None else total + d
        projected[:, cols] = total
        squares = squares + jnp.sum(total * total, axis=-1, keepdims=True)
    scale = lax.rsqrt(squares * (1.0 / WIDTH) + EPS)
    out[0] = (projected[...] * scale * out_gain[...]).astype(BF16)

    for copy in sent:
        copy.wait_send()


def on_device(tokens, in_gain, wq, wk, wv, q_gain, k_gain, wo, out_gain):
    vmem = pl.BlockSpec(memory_space=pltpu.VMEM)
    dma = pltpu.SemaphoreType.DMA
    return pl.pallas_call(
        kernel,
        out_shape=jax.ShapeDtypeStruct((1, ROWS, WIDTH), BF16),
        in_specs=[vmem] * 9,
        out_specs=vmem,
        scratch_shapes=[
            pltpu.VMEM((3, ROWS, WIDTH), BF16),
            pltpu.VMEM((GROUP, ROWS, WIDTH), BF16),
            pltpu.VMEM((2 * Z, SHARD, CUT), BF16),
            pltpu.VMEM((2 * Z, SHARD, WIDTH), BF16),
            pltpu.VMEM((GROUP, ROWS, HEAD), F32),
            pltpu.VMEM((GROUP, ROWS, HEAD), F32),
            pltpu.VMEM((2 * HEAD, KEYS * GROUP), BF16),
            pltpu.VMEM((GROUP, KEYS, HEAD), BF16),
            pltpu.VMEM((GROUP, HEAD + ONES, KEYS), BF16),
            pltpu.VMEM((KEYS, BQ), F32),
            pltpu.VMEM((KEYS, BQ), F32),
            pltpu.VMEM((8, BQ), F32),
            pltpu.VMEM((8, BQ), F32),
            pltpu.VMEM((1, KEYS * GROUP), F32),
            pltpu.VMEM((HEAD + ONES, KEYS * GROUP), F32),
            pltpu.VMEM((GROUP, ROWS, 512), BF16),
            pltpu.VMEM((GROUP, ROWS, 512), BF16),
            pltpu.VMEM((ROWS, WIDTH), F32),
            dma((6,)),
            dma((6,)),
            dma((2, 4, 2)),
            dma((2, 4, 2)),
            dma((Z, 2)),
            dma((Z, 2)),
            dma((2, 4, 2)),
            dma((2, 4, 2)),
            dma((Z, 2)),
            dma((Z, 2)),
            dma((6,)),
            dma((6,)),
            dma((3,)),
            dma((3,)),
        ],
        compiler_params=pltpu.CompilerParams(
            collective_id=0, has_side_effects=True, vmem_limit_bytes=60 * 2**20
        ),
        name="grouped_attention",
    )(
        tokens,
        in_gain.reshape(1, WIDTH),
        wq,
        wk,
        wv,
        q_gain.reshape(1, HEAD),
        k_gain.reshape(1, HEAD),
        wo,
        out_gain.reshape(1, WIDTH),
    )


def solution(mesh):
    placed = (
        P("dp", "sp", None),
        P(),
        P("dp", None),
        P("dp", None),
        P("dp", None),
        P(),
        P(),
        P("dp", None),
        P(),
    )
    return jax.shard_map(
        on_device, mesh=mesh, in_specs=placed, out_specs=P("dp", "sp", None), check_vma=False
    )
```

```python
import jax
import jax.numpy as jnp
from jax import lax
from jax.experimental import pallas as pl
from jax.experimental.pallas import tpu as pltpu
from jax.sharding import PartitionSpec as P

MESH = pl.DeviceIdType.MESH
F32 = jnp.float32
BF16 = jnp.bfloat16

EPS = 1e-06
THETA = 10000.0
GRID_W = 64
HEAD = 128
WIDTH = 2048
ROWS = 256
GROUP = 4
KEYS = GROUP * ROWS
Z = 8
SHARD = WIDTH // (2 * Z)
NEAR = 1280
SHARED = 512
FAR = 768
HALF = ROWS // 2
BQ = 512
TILES = KEYS * GROUP // BQ
ONES = 16
LOG2E = 1.4426950408889634


def span(index, size):
    return pl.ds(pl.multiple_of(index * size, size), size)


def kernel(
    tokens_in,
    in_gain,
    wq_in,
    wk_in,
    wv_in,
    q_gain,
    k_gain,
    wo_in,
    out_gain,
    out,
    tokens,
    wq,
    wk,
    wv,
    wo,
    raw,
    normed,
    kv_weights,
    q_weights,
    near,
    far,
    cosines,
    sines,
    qt,
    kbuf,
    vbuf,
    s0,
    s1,
    top0,
    top1,
    row_max,
    acc,
    attended,
    returned,
    projected,
    in_sem,
    ag_send,
    ag_recv,
    zk_send,
    zk_recv,
    ck_send,
    ck_recv,
    zq_send,
    zq_recv,
    cq_send,
    cq_recv,
    zo_send,
    zo_recv,
    co_send,
    co_recv,
    far_send,
    far_recv,
    cf_send,
    cf_recv,
    kv_send,
    kv_recv,
    ret_send,
    ret_recv,
):
    staged = []
    for i, (src, dst) in enumerate(
        ((tokens_in.at[0], tokens), (wk_in, wk), (wv_in, wv), (wq_in, wq), (wo_in, wo))
    ):
        staged.append(pltpu.make_async_copy(src, dst, in_sem.at[i]))
        staged[-1].start()

    sp = lax.axis_index("sp")
    dp = lax.axis_index("dp")
    y, x = sp // 4, sp % 4
    z, core = dp // 2, dp % 2
    at = (1 - core) * y + core * x
    group = (y + x) % 4
    side = group % 2

    def member(step):
        to = (at + step) % 4
        return (1 - core) * (to * 4 + x) + core * (y * 4 + to)

    def diagonal(step):
        return ((y + 4 - step) % 4) * 4 + (x + step) % 4

    up = {"dp": ((z + 1) % Z) * 2 + core}
    down = {"dp": ((z + Z - 1) % Z) * 2 + core}
    twin = {"dp": z * 2 + 1 - core}
    peers = [{"sp": member(1)}, {"sp": member(3)}, {"sp": member(2)}]
    peers += [{"sp": diagonal(1)}, {"sp": diagonal(3)}, up, down, twin]

    barrier = pltpu.get_barrier_semaphore()
    for peer in peers:
        pl.semaphore_signal(barrier, inc=1, device_id=peer, device_id_type=MESH)
    for copy in staged:
        copy.wait()
    pl.semaphore_wait(barrier, len(peers))

    sent = []

    def send(src, dst, send_sem, recv_sem, to):
        copy = pltpu.make_async_remote_copy(
            src_ref=src,
            dst_ref=dst,
            send_sem=send_sem,
            recv_sem=recv_sem,
            device_id=to,
            device_id_type=MESH,
        )
        copy.start()
        return copy

    def send_parts(pairs, whole, send_sem, recv_sem, to):
        for src, dst in pairs:
            send(src, dst, send_sem, recv_sem, to)
        sent.append(
            pltpu.make_async_remote_copy(
                src_ref=whole,
                dst_ref=whole,
                send_sem=send_sem,
                recv_sem=recv_sem,
                device_id=to,
                device_id_type=MESH,
            )
        )

    def arrival(ref, sem):
        pltpu.make_async_copy(ref, ref, sem).wait()

    low, high = pl.ds(0, HALF), pl.ds(HALF, HALF)
    nxt, prv = {"sp": member(1)}, {"sp": member(3)}

    def token_send(src, slot, part, index, to):
        sent.append(
            send(src, raw.at[slot - 1, part], ag_send.at[index], ag_recv.at[index], to)
        )

    token_send(tokens.at[low], 3, low, 0, nxt)
    token_send(tokens.at[high], 1, high, 1, prv)
    token_send(tokens.at[high], 3, high, 2, nxt)
    token_send(tokens.at[low], 1, low, 3, prv)

    chunks = (pl.ds(0, SHARD // 2), pl.ds(SHARD // 2, SHARD // 2))
    q_cols = span(group, 512)
    kv_cols = span(group, HEAD)
    side_cols = pl.ds(pl.multiple_of(SHARED + side * FAR, 256), FAR)
    other_cols = pl.ds(pl.multiple_of(SHARED + (1 - side) * FAR, 256), FAR)

    def kv_parts(i):
        mine = kv_weights.at[dp, chunks[i]]
        pairs = [
            (wk.at[chunks[i], kv_cols], mine.at[:, pl.ds(0, HEAD)]),
            (wv.at[chunks[i], kv_cols], mine.at[:, pl.ds(HEAD, HEAD)]),
        ]
        return pairs, mine

    def q_parts(i):
        mine = q_weights.at[dp, chunks[i]]
        return [(wq.at[chunks[i], q_cols], mine)], mine

    def near_parts(i):
        mine = near.at[dp, chunks[i]]
        pairs = [
            (wo.at[chunks[i], pl.ds(0, SHARED)], mine.at[:, pl.ds(0, SHARED)]),
            (wo.at[chunks[i], side_cols], mine.at[:, pl.ds(SHARED, FAR)]),
        ]
        return pairs, mine

    def ring_start(parts, zs, zr):
        for i in (0, 1):
            for way, to in ((0, up), (1, down)):
                send_parts(*parts(i), zs.at[way, 0, i], zr.at[way, 0, i], to)

    def twin_start(parts, cs, cr):
        for i in (0, 1):
            send_parts(*parts(i), cs.at[0, i], cr.at[0, i], twin)

    def source_of(way, step):
        return (((z + Z - step) % Z) if way == 0 else ((z + step) % Z)) * 2 + core

    def slot_of(way, step):
        return step if way == 0 else Z - step

    def ring_event(buf, zs, zr, cs, cr, way, step, i):
        part = buf.at[source_of(way, step), chunks[i]]
        arrival(part, zr.at[way, step - 1, i])
        if step < 3 or (step == 3 and i == way):
            sent.append(
                send(part, part, zs.at[way, step, i], zr.at[way, step, i], (up, down)[way])
            )
        slot = slot_of(way, step)
        sent.append(send(part, part, cs.at[slot, i], cr.at[slot, i], twin))

    def ring_events(ring, step, which=(0, 1)):
        for i in which:
            for way in (0, 1):
                if step < 4 or i == way:
                    ring_event(*ring, way, step, i)

    def twin_arrivals(buf, cr, first=0):
        for slot in range(first, Z):
            source = ((z + Z - slot) % Z) * 2 + 1 - core
            for i in (0, 1):
                arrival(buf.at[source, chunks[i]], cr.at[slot, i])

    kv_ring = (kv_weights, zk_send, zk_recv, ck_send, ck_recv)
    q_ring = (q_weights, zq_send, zq_recv, cq_send, cq_recv)
    near_ring = (near, zo_send, zo_recv, co_send, co_recv)

    ring_start(kv_parts, zk_send, zk_recv)
    ring_start(q_parts, zq_send, zq_recv)
    twin_start(kv_parts, ck_send, ck_recv)
    twin_start(q_parts, cq_send, cq_recv)

    kv_weights[dp, :, 0:HEAD] = wk[:, kv_cols]
    kv_weights[dp, :, HEAD : 2 * HEAD] = wv[:, kv_cols]
    q_weights[dp] = wq[:, q_cols]
    near[dp, :, 0:SHARED] = wo[:, 0:SHARED]
    near[dp, :, SHARED:NEAR] = wo[:, side_cols]
    far[dp] = wo[:, other_cols]

    gain_in = in_gain[...]

    def normalize(src, slot):
        def rows(i, c):
            part = pl.ds(pl.multiple_of(i * 32, 32), 32)
            v = src[part, :].astype(F32)
            ms = jnp.mean(v * v, axis=-1, keepdims=True)
            normed[slot, part, :] = (v * lax.rsqrt(ms + EPS) * gain_in).astype(BF16)
            return c

        lax.fori_loop(0, ROWS // 32, rows, 0)

    def angles(slot, c):
        row = lax.broadcasted_iota(jnp.int32, (ROWS, HEAD), 0)
        lane = lax.broadcasted_iota(jnp.int32, (ROWS, HEAD), 1)
        power = (lane % 32).astype(F32) * (1.0 / 32.0)
        freq = jnp.exp(power * (-9.210340371976184))
        grid_row = member(slot) * (ROWS // GRID_W) + row // GRID_W
        place = jnp.where(lane < 64, grid_row, row % GRID_W).astype(F32)
        angle = place * freq
        cosines[slot] = jnp.cos(angle)
        sine = jnp.sin(angle)
        sines[slot] = jnp.where(lane % 64 < 32, -sine, sine)
        return c

    normalize(tokens, 0)
    ring_events(kv_ring, 1)
    ring_events(q_ring, 1)
    ring_events(kv_ring, 2)
    arrival(raw.at[2, low], ag_recv.at[0])
    token_send(raw.at[2, low], 2, low, 4, nxt)
    arrival(raw.at[0, high], ag_recv.at[1])
    token_send(raw.at[0, high], 2, high, 5, prv)
    ring_events(q_ring, 2)
    lax.fori_loop(0, GROUP, angles, 0)
    ring_events(kv_ring, 3)
    ring_events(q_ring, 3)
    arrival(raw.at[2, high], ag_recv.at[2])
    arrival(raw.at[0, low], ag_recv.at[3])
    normalize(raw.at[0], 1)
    ring_events(kv_ring, 4)
    normalize(raw.at[2], 3)
    ring_events(q_ring, 4)
    ring_start(near_parts, zo_send, zo_recv)
    twin_arrivals(kv_weights, ck_recv)

    gain_q, gain_k = q_gain[...], k_gain[...]
    lane_of = lax.broadcasted_iota(jnp.int32, (ROWS, HEAD), 1)
    first = lane_of % 64 < 32

    def finish(v, gain, slot):
        ms = jnp.mean(v * v, axis=-1, keepdims=True)
        v = v * lax.rsqrt(ms + EPS) * gain
        other = jnp.where(first, pltpu.roll(v, HEAD - 32, 1), pltpu.roll(v, 32, 1))
        return v * cosines[slot] + other * sines[slot]

    def project_kv(slot):
        cut = kv_weights[...].reshape(WIDTH, 2 * HEAD)
        values = jnp.dot(normed[slot], cut, preferred_element_type=F32)
        rows = pl.ds(slot * ROWS, ROWS)
        kbuf[0, rows, :] = finish(values[:, 0:HEAD], gain_k, slot).astype(BF16)
        vbuf[0, 0:HEAD, rows] = values[:, HEAD : 2 * HEAD].T.astype(BF16)

    def kv_part(d, what, half):
        part = pl.ds(half * KEYS // 2, KEYS // 2)
        return kbuf.at[d, part] if what == 0 else vbuf.at[d, pl.ds(0, HEAD), part]

    def kv_index(d, what, half):
        return (d - 1) * 4 + what * 2 + half

    def kv_send_to(src, slot, what, half, to):
        index = kv_index(slot, what, half)
        sent.append(
            send(
                kv_part(src, what, half),
                kv_part(slot, what, half),
                kv_send.at[index],
                kv_recv.at[index],
                {"sp": diagonal(to)},
            )
        )

    def kv_arrival(slot, what, half):
        arrival(kv_part(slot, what, half), kv_recv.at[kv_index(slot, what, half)])

    def kv_out(half):
        kv_send_to(0, 3, 0, half, 1)
        kv_send_to(0, 1, 1, half, 3)
        kv_send_to(0, 3, 1, half, 1)
        kv_send_to(0, 1, 0, half, 3)

    def kv_pass(half):
        kv_arrival(3, 0, half)
        kv_send_to(3, 2, 0, half, 1)
        kv_arrival(1, 1, half)
        kv_send_to(1, 2, 1, half, 3)

    project_kv(0)
    project_kv(1)
    kv_out(0)
    arrival(raw.at[1, low], ag_recv.at[4])
    arrival(raw.at[1, high], ag_recv.at[5])
    normalize(raw.at[1], 2)
    project_kv(3)
    project_kv(2)
    kv_out(1)
    twin_arrivals(q_weights, cq_recv)
    twin_start(near_parts, co_send, co_recv)
    for i in (0, 1):
        part = far.at[dp, chunks[i]]
        sent.append(
            send(wo.at[chunks[i], other_cols], part, cf_send.at[0, i], cf_recv.at[0, i], twin)
        )

    def project_q(slot, c):
        cut = q_weights[...].reshape(WIDTH, 512)
        values = jnp.dot(normed[slot], cut, preferred_element_type=F32)
        for h in range(4):
            q = finish(values[:, h * HEAD : (h + 1) * HEAD], gain_q, slot)
            q = q.astype(BF16).astype(F32).T * (HEAD**-0.5 * LOG2E)
            coarse = q.astype(BF16)
            fine = (q - coarse.astype(F32)).astype(BF16)
            cols = pl.ds(pl.multiple_of(slot * KEYS + h * ROWS, ROWS), ROWS)
            qt[0:HEAD, cols] = coarse
            qt[HEAD : 2 * HEAD, cols] = fine
        return c

    lax.fori_loop(0, GROUP, project_q, 0)

    def far_out(step, i):
        for way in (0, 1):
            if step < 4 or i == way:
                source, slot = source_of(way, step), slot_of(way, step)
                sent.append(
                    send(
                        near.at[source, chunks[i], pl.ds(SHARED, FAR)],
                        far.at[source, chunks[i]],
                        far_send.at[slot, i],
                        far_recv.at[slot, i],
                        (nxt, prv)[i],
                    )
                )

    def far_pass(step, i):
        for way in (0, 1):
            if step < 4 or i == way:
                slot = slot_of(way, step)
                part = far.at[source_of(way, step), chunks[i]]
                arrival(part, far_recv.at[slot, i])
                sent.append(send(part, part, cf_send.at[slot, i], cf_recv.at[slot, i], twin))

    ones = jnp.ones((ONES, KEYS), BF16)
    for d in range(GROUP):
        vbuf[d, HEAD : HEAD + ONES, :] = ones
    row_max[...] = jnp.full_like(row_max, -1e30)
    acc[...] = jnp.zeros_like(acc)
    size = 256

    def attend(nt, sn, topn, next_keys, ct, sc, topc, keys):
        if sc is not None:
            cols = span(ct, BQ)
            old = row_max[:, cols]
            new = jnp.maximum(old, jnp.max(topc[...], axis=0, keepdims=True))
            row_max[:, cols] = new
            decay = jnp.exp2(old - new)
        top, total = None, None
        for c in range(KEYS // size):
            part = pl.ds(c * size, size)
            if sn is not None:
                d, begin = next_keys[c]
                k = kbuf[d, pl.ds(begin, size), :]
                s = jnp.dot(
                    jnp.concatenate([k, k], axis=1),
                    qt[:, span(nt, BQ)],
                    preferred_element_type=F32,
                )
                sn[part, :] = s
                most = jnp.max(s.reshape(size // 8, 8, BQ), axis=0)
                top = most if top is None else jnp.maximum(top, most)
            if sc is not None:
                d, begin = keys[c]
                p = jnp.exp2(sc[part, :] - new).astype(BF16)
                v = jnp.dot(
                    vbuf[d, :, pl.ds(begin, size)], p, preferred_element_type=F32
                )
                total = v if total is None else total + v
        if sn is not None:
            topn[...] = top
        if sc is not None:
            acc[:, cols] = acc[:, cols] * decay + total

    def attend_block(keys, next_keys, middle, late):
        def pair(i, c):
            t = i * 2
            attend(t + 1, s1, top1, keys, t, s0, top0, keys)
            attend(t + 2, s0, top0, keys, t + 1, s1, top1, keys)
            return c

        lax.fori_loop(0, TILES // 4, pair, 0)
        middle()
        lax.fori_loop(TILES // 4, TILES // 2 - 1, pair, 0)
        late()
        t = TILES - 2
        attend(t + 1, s1, top1, keys, t, s0, top0, keys)
        if next_keys is None:
            attend(None, None, None, None, t + 1, s1, top1, keys)
        else:
            attend(0, s0, top0, next_keys, t + 1, s1, top1, keys)

    quarters = [i * size for i in range(KEYS // size)]
    own = [(0, i) for i in quarters]
    firsts = [(3, i) for i in quarters[:2]] + [(1, i) for i in quarters[:2]]
    seconds = [(3, i) for i in quarters[2:]] + [(1, i) for i in quarters[2:]]
    opposite = [(2, i) for i in quarters]

    attend(0, s0, top0, own, None, None, None, None)

    def middle0():
        ring_events(near_ring, 1, (0,))

    def late0():
        kv_pass(0)
        kv_arrival(3, 1, 0)
        kv_arrival(1, 0, 0)

    attend_block(own, firsts, middle0, late0)
    ring_events(near_ring, 1, (1,))

    def middle1():
        ring_events(near_ring, 2, (0,))

    def late1():
        kv_pass(1)
        kv_arrival(3, 1, 1)
        kv_arrival(1, 0, 1)
        far_out(1, 0)
        far_out(1, 1)

    attend_block(firsts, seconds, middle1, late1)

    def middle2():
        ring_events(near_ring, 2, (1,))
        far_out(2, 0)
        far_out(2, 1)

    def late2():
        ring_events(near_ring, 3, (0,))
        for half in (0, 1):
            kv_arrival(2, 0, half)
            kv_arrival(2, 1, half)

    attend_block(seconds, opposite, middle2, late2)

    def middle3():
        far_out(3, 0)

    def late3():
        ring_events(near_ring, 3, (1,))
        far_out(3, 1)
        for i in (0, 1):
            far_pass(1, i)

    attend_block(opposite, None, middle3, late3)

    def hand_back(slot):
        for h in range(4):
            cols = pl.ds(slot * KEYS + h * ROWS, ROWS)
            scaled = acc[0:HEAD, cols] / acc[HEAD : HEAD + 1, cols]
            attended[slot, :, h * HEAD : (h + 1) * HEAD] = scaled.T.astype(BF16)

    for slot in (2, 1, 3):
        hand_back(slot)
        sent.append(
            send(
                attended.at[slot],
                returned.at[group],
                ret_send.at[slot - 1],
                ret_recv.at[slot - 1],
                {"sp": member(slot)},
            )
        )
    hand_back(0)
    returned[group] = attended[0]
    ring_events(near_ring, 4)
    far_out(4, 0)
    far_out(4, 1)
    for step in (2, 3, 4):
        for i in (0, 1):
            far_pass(step, i)
    for slot in (1, 2, 3):
        arrival(returned.at[(group + 4 - slot) % 4], ret_recv.at[slot - 1])
    twin_arrivals(near, co_recv)

    def project_out(buf, begin, width):
        total = None
        for g in range(4):
            w = buf[g * 4 : (g + 1) * 4, :, begin : begin + width].reshape(512, width)
            d = jnp.dot(returned[g], w, preferred_element_type=F32)
            total = d if total is None else total + d
        return total, jnp.sum(total * total, axis=-1, keepdims=True)

    total, squares = project_out(near, 0, SHARED)
    projected[:, 0:SHARED] = total
    total, more = project_out(near, SHARED, FAR)
    projected[:, side_cols] = total
    squares = squares + more
    twin_arrivals(far, cf_recv)
    total, more = project_out(far, 0, FAR)
    projected[:, other_cols] = total
    squares = squares + more
    scale = lax.rsqrt(squares * (1.0 / WIDTH) + EPS)
    out[0] = (projected[...] * scale * out_gain[...]).astype(BF16)

    for copy in sent:
        copy.wait_send()


def on_device(tokens, in_gain, wq, wk, wv, q_gain, k_gain, wo, out_gain):
    vmem = pl.BlockSpec(memory_space=pltpu.VMEM)
    hbm = pl.BlockSpec(memory_space=pl.ANY)
    dma = pltpu.SemaphoreType.DMA
    ring, other_core = dma((2, 4, 2)), dma((Z, 2))
    return pl.pallas_call(
        kernel,
        out_shape=jax.ShapeDtypeStruct((1, ROWS, WIDTH), BF16),
        in_specs=[hbm, vmem, hbm, hbm, hbm, vmem, vmem, hbm, vmem],
        out_specs=vmem,
        scratch_shapes=[
            pltpu.VMEM((ROWS, WIDTH), BF16),
            pltpu.VMEM(wq.shape, BF16),
            pltpu.VMEM(wk.shape, BF16),
            pltpu.VMEM(wv.shape, BF16),
            pltpu.VMEM(wo.shape, BF16),
            pltpu.VMEM((3, ROWS, WIDTH), BF16),
            pltpu.VMEM((GROUP, ROWS, WIDTH), BF16),
            pltpu.VMEM((2 * Z, SHARD, 2 * HEAD), BF16),
            pltpu.VMEM((2 * Z, SHARD, 512), BF16),
            pltpu.VMEM((2 * Z, SHARD, NEAR), BF16),
            pltpu.VMEM((2 * Z, SHARD, FAR), BF16),
            pltpu.VMEM((GROUP, ROWS, HEAD), F32),
            pltpu.VMEM((GROUP, ROWS, HEAD), F32),
            pltpu.VMEM((2 * HEAD, KEYS * GROUP), BF16),
            pltpu.VMEM((GROUP, KEYS, HEAD), BF16),
            pltpu.VMEM((GROUP, HEAD + ONES, KEYS), BF16),
            pltpu.VMEM((KEYS, BQ), F32),
            pltpu.VMEM((KEYS, BQ), F32),
            pltpu.VMEM((8, BQ), F32),
            pltpu.VMEM((8, BQ), F32),
            pltpu.VMEM((1, KEYS * GROUP), F32),
            pltpu.VMEM((HEAD + ONES, KEYS * GROUP), F32),
            pltpu.VMEM((GROUP, ROWS, 512), BF16),
            pltpu.VMEM((GROUP, ROWS, 512), BF16),
            pltpu.VMEM((ROWS, WIDTH), F32),
            dma((5,)),
            dma((6,)),
            dma((6,)),
            *([ring, ring, other_core, other_core] * 3),
            *([other_core] * 4),
            dma((12,)),
            dma((12,)),
            dma((3,)),
            dma((3,)),
        ],
        compiler_params=pltpu.CompilerParams(
            collective_id=0, has_side_effects=True, vmem_limit_bytes=60 * 2**20
        ),
        name="grouped_attention",
    )(
        tokens,
        in_gain.reshape(1, WIDTH),
        wq,
        wk,
        wv,
        q_gain.reshape(1, HEAD),
        k_gain.reshape(1, HEAD),
        wo,
        out_gain.reshape(1, WIDTH),
    )


def solution(mesh):
    placed = (
        P("dp", "sp", None),
        P(),
        P("dp", None),
        P("dp", None),
        P("dp", None),
        P(),
        P(),
        P("dp", None),
        P(),
    )
    return jax.shard_map(
        on_device, mesh=mesh, in_specs=placed, out_specs=P("dp", "sp", None), check_vma=False
    )
```

```python
import jax
import jax.numpy as jnp
from jax import lax
from jax.experimental import pallas as pl
from jax.experimental.pallas import tpu as pltpu
from jax.sharding import PartitionSpec as P

MESH = pl.DeviceIdType.MESH
F32 = jnp.float32
BF16 = jnp.bfloat16

EPS = 1e-06
THETA = 10000.0
GRID_W = 64
HEAD = 128
WIDTH = 2048
ROWS = 256
GROUP = 4
KEYS = GROUP * ROWS
Z = 8
SHARD = WIDTH // (2 * Z)
NEAR = 1280
SHARED = 512
FAR = 768
HALF = ROWS // 2
BQ = 512
TILES = KEYS * GROUP // BQ
ONES = 16
LOG2E = 1.4426950408889634


def span(index, size):
    return pl.ds(pl.multiple_of(index * size, size), size)


def kernel(
    tokens_in,
    in_gain_in,
    wq_in,
    wk_in,
    wv_in,
    q_gain_in,
    k_gain_in,
    wo_in,
    out_gain_in,
    out,
    in_gain,
    q_gain,
    k_gain,
    out_gain,
    tokens,
    wq,
    wk,
    wv,
    wo,
    raw,
    normed,
    kv_weights,
    q_weights,
    near,
    far,
    cosines,
    sines,
    cosines_t,
    sines_t,
    qt,
    kbuf,
    vbuf,
    s0,
    s1,
    top0,
    top1,
    row_max,
    acc,
    attended,
    returned,
    projected,
    in_sem,
    ag_send,
    ag_recv,
    zk_send,
    zk_recv,
    ck_send,
    ck_recv,
    zq_send,
    zq_recv,
    cq_send,
    cq_recv,
    zo_send,
    zo_recv,
    co_send,
    co_recv,
    far_send,
    far_recv,
    cf_send,
    cf_recv,
    kv_send,
    kv_recv,
    ret_send,
    ret_recv,
):
    staged = []
    for i, (src, dst) in enumerate(
        (
            (tokens_in.at[0], tokens),
            (wk_in, wk),
            (wv_in, wv),
            (wq_in, wq),
            (wo_in, wo),
            (in_gain_in, in_gain),
            (q_gain_in, q_gain),
            (k_gain_in, k_gain),
            (out_gain_in, out_gain),
        )
    ):
        staged.append(pltpu.make_async_copy(src, dst, in_sem.at[i]))
        staged[-1].start()

    sp = lax.axis_index("sp")
    dp = lax.axis_index("dp")
    y, x = sp // 4, sp % 4
    z, core = dp // 2, dp % 2
    at = (1 - core) * y + core * x
    group = (y + x) % 4
    side = group % 2

    def member(step):
        to = (at + step) % 4
        return (1 - core) * (to * 4 + x) + core * (y * 4 + to)

    def diagonal(step):
        return ((y + 4 - step) % 4) * 4 + (x + step) % 4

    up = {"dp": ((z + 1) % Z) * 2 + core}
    down = {"dp": ((z + Z - 1) % Z) * 2 + core}
    twin = {"dp": z * 2 + 1 - core}
    peers = [{"sp": member(1)}, {"sp": member(3)}, {"sp": member(2)}]
    peers += [{"sp": diagonal(1)}, {"sp": diagonal(3)}, up, down, twin]

    barrier = pltpu.get_barrier_semaphore()
    for peer in peers:
        pl.semaphore_signal(barrier, inc=1, device_id=peer, device_id_type=MESH)
    for copy in staged[:4]:
        copy.wait()
    pl.semaphore_wait(barrier, len(peers))

    sent = []

    def send(src, dst, send_sem, recv_sem, to):
        copy = pltpu.make_async_remote_copy(
            src_ref=src,
            dst_ref=dst,
            send_sem=send_sem,
            recv_sem=recv_sem,
            device_id=to,
            device_id_type=MESH,
        )
        copy.start()
        return copy

    def send_parts(pairs, whole, send_sem, recv_sem, to):
        for src, dst in pairs:
            send(src, dst, send_sem, recv_sem, to)
        sent.append(
            pltpu.make_async_remote_copy(
                src_ref=whole,
                dst_ref=whole,
                send_sem=send_sem,
                recv_sem=recv_sem,
                device_id=to,
                device_id_type=MESH,
            )
        )

    def arrival(ref, sem):
        pltpu.make_async_copy(ref, ref, sem).wait()

    low, high = pl.ds(0, HALF), pl.ds(HALF, HALF)
    nxt, prv = {"sp": member(1)}, {"sp": member(3)}

    def token_send(src, slot, part, index, to):
        sent.append(
            send(src, raw.at[slot - 1, part], ag_send.at[index], ag_recv.at[index], to)
        )

    token_send(tokens.at[low], 3, low, 0, nxt)
    token_send(tokens.at[high], 1, high, 1, prv)
    token_send(tokens.at[high], 3, high, 2, nxt)
    token_send(tokens.at[low], 1, low, 3, prv)

    chunks = (pl.ds(0, SHARD // 2), pl.ds(SHARD // 2, SHARD // 2))
    q_cols = span(group, 512)
    kv_cols = span(group, HEAD)
    side_cols = pl.ds(pl.multiple_of(SHARED + side * FAR, 256), FAR)
    other_cols = pl.ds(pl.multiple_of(SHARED + (1 - side) * FAR, 256), FAR)

    def kv_parts(i):
        mine = kv_weights.at[dp, chunks[i]]
        pairs = [
            (wk.at[chunks[i], kv_cols], mine.at[:, pl.ds(0, HEAD)]),
            (wv.at[chunks[i], kv_cols], mine.at[:, pl.ds(HEAD, HEAD)]),
        ]
        return pairs, mine

    def q_parts(i):
        mine = q_weights.at[dp, chunks[i]]
        return [(wq.at[chunks[i], q_cols], mine)], mine

    def near_parts(i):
        mine = near.at[dp, chunks[i]]
        pairs = [
            (wo.at[chunks[i], pl.ds(0, SHARED)], mine.at[:, pl.ds(0, SHARED)]),
            (wo.at[chunks[i], side_cols], mine.at[:, pl.ds(SHARED, FAR)]),
        ]
        return pairs, mine

    def ring_start(parts, zs, zr):
        for i in (0, 1):
            for way, to in ((0, up), (1, down)):
                send_parts(*parts(i), zs.at[way, 0, i], zr.at[way, 0, i], to)

    def twin_start(parts, cs, cr):
        for i in (0, 1):
            send_parts(*parts(i), cs.at[0, i], cr.at[0, i], twin)

    def source_of(way, step):
        return (((z + Z - step) % Z) if way == 0 else ((z + step) % Z)) * 2 + core

    def slot_of(way, step):
        return step if way == 0 else Z - step

    def ring_event(buf, zs, zr, cs, cr, way, step, i):
        part = buf.at[source_of(way, step), chunks[i]]
        arrival(part, zr.at[way, step - 1, i])
        if step < 3 or (step == 3 and i == way):
            sent.append(
                send(part, part, zs.at[way, step, i], zr.at[way, step, i], (up, down)[way])
            )
        slot = slot_of(way, step)
        sent.append(send(part, part, cs.at[slot, i], cr.at[slot, i], twin))

    def ring_events(ring, step, which=(0, 1)):
        for i in which:
            for way in (0, 1):
                if step < 4 or i == way:
                    ring_event(*ring, way, step, i)

    def twin_arrivals(buf, cr, first=0):
        for slot in range(first, Z):
            source = ((z + Z - slot) % Z) * 2 + 1 - core
            for i in (0, 1):
                arrival(buf.at[source, chunks[i]], cr.at[slot, i])

    kv_ring = (kv_weights, zk_send, zk_recv, ck_send, ck_recv)
    q_ring = (q_weights, zq_send, zq_recv, cq_send, cq_recv)
    near_ring = (near, zo_send, zo_recv, co_send, co_recv)

    ring_start(kv_parts, zk_send, zk_recv)
    ring_start(q_parts, zq_send, zq_recv)
    twin_start(kv_parts, ck_send, ck_recv)
    twin_start(q_parts, cq_send, cq_recv)

    for copy in staged[4:]:
        copy.wait()
    kv_weights[dp, :, 0:HEAD] = wk[:, kv_cols]
    kv_weights[dp, :, HEAD : 2 * HEAD] = wv[:, kv_cols]
    q_weights[dp] = wq[:, q_cols]
    near[dp, :, 0:SHARED] = wo[:, 0:SHARED]
    near[dp, :, SHARED:NEAR] = wo[:, side_cols]
    far[dp] = wo[:, other_cols]

    gain_in = in_gain[...]

    def normalize(src, slot):
        def rows(i, c):
            part = pl.ds(pl.multiple_of(i * 32, 32), 32)
            v = src[part, :].astype(F32)
            ms = jnp.mean(v * v, axis=-1, keepdims=True)
            normed[slot, part, :] = (v * lax.rsqrt(ms + EPS) * gain_in).astype(BF16)
            return c

        lax.fori_loop(0, ROWS // 32, rows, 0)

    def angles(slot, c):
        row = lax.broadcasted_iota(jnp.int32, (ROWS, HEAD), 0)
        lane = lax.broadcasted_iota(jnp.int32, (ROWS, HEAD), 1)
        power = (lane % 32).astype(F32) * (1.0 / 32.0)
        freq = jnp.exp(power * (-9.210340371976184))
        grid_row = member(slot) * (ROWS // GRID_W) + row // GRID_W
        place = jnp.where(lane < 64, grid_row, row % GRID_W).astype(F32)
        angle = place * freq
        cosine = jnp.cos(angle)
        sine = jnp.sin(angle)
        sine = jnp.where(lane % 64 < 32, -sine, sine)
        cosines[slot] = cosine
        sines[slot] = sine
        cosines_t[slot] = cosine.T
        sines_t[slot] = sine.T
        return c

    normalize(tokens, 0)
    ring_events(kv_ring, 1)
    ring_events(q_ring, 1)
    ring_events(kv_ring, 2)
    arrival(raw.at[2, low], ag_recv.at[0])
    token_send(raw.at[2, low], 2, low, 4, nxt)
    arrival(raw.at[0, high], ag_recv.at[1])
    token_send(raw.at[0, high], 2, high, 5, prv)
    ring_events(q_ring, 2)
    lax.fori_loop(0, GROUP, angles, 0)
    ring_events(kv_ring, 3)
    ring_events(q_ring, 3)
    arrival(raw.at[2, high], ag_recv.at[2])
    arrival(raw.at[0, low], ag_recv.at[3])
    normalize(raw.at[0], 1)
    ring_events(kv_ring, 4)
    normalize(raw.at[2], 3)
    ring_events(q_ring, 4)
    ring_start(near_parts, zo_send, zo_recv)
    twin_arrivals(kv_weights, ck_recv)

    gain_q, gain_k = q_gain[...], k_gain[...]
    lane_of = lax.broadcasted_iota(jnp.int32, (ROWS, HEAD), 1)
    first = lane_of % 64 < 32

    def finish(v, gain, slot):
        ms = jnp.mean(v * v, axis=-1, keepdims=True)
        v = v * lax.rsqrt(ms + EPS) * gain
        other = jnp.where(first, pltpu.roll(v, HEAD - 32, 1), pltpu.roll(v, 32, 1))
        return v * cosines[slot] + other * sines[slot]

    def project_kv(slot):
        cut = kv_weights[...].reshape(WIDTH, 2 * HEAD)
        values = jnp.dot(normed[slot], cut, preferred_element_type=F32)
        rows = pl.ds(slot * ROWS, ROWS)
        kbuf[0, rows, :] = finish(values[:, 0:HEAD], gain_k, slot).astype(BF16)
        vbuf[0, 0:HEAD, rows] = values[:, HEAD : 2 * HEAD].T.astype(BF16)

    def kv_part(d, what, half):
        part = pl.ds(half * KEYS // 2, KEYS // 2)
        return kbuf.at[d, part] if what == 0 else vbuf.at[d, pl.ds(0, HEAD), part]

    def kv_index(d, what, half):
        return (d - 1) * 4 + what * 2 + half

    def kv_send_to(src, slot, what, half, to):
        index = kv_index(slot, what, half)
        sent.append(
            send(
                kv_part(src, what, half),
                kv_part(slot, what, half),
                kv_send.at[index],
                kv_recv.at[index],
                {"sp": diagonal(to)},
            )
        )

    def kv_arrival(slot, what, half):
        arrival(kv_part(slot, what, half), kv_recv.at[kv_index(slot, what, half)])

    def kv_out(half):
        kv_send_to(0, 3, 0, half, 1)
        kv_send_to(0, 1, 1, half, 3)
        kv_send_to(0, 3, 1, half, 1)
        kv_send_to(0, 1, 0, half, 3)

    def kv_pass(half):
        kv_arrival(3, 0, half)
        kv_send_to(3, 2, 0, half, 1)
        kv_arrival(1, 1, half)
        kv_send_to(1, 2, 1, half, 3)

    project_kv(0)
    project_kv(1)
    kv_out(0)
    arrival(raw.at[1, low], ag_recv.at[4])
    arrival(raw.at[1, high], ag_recv.at[5])
    normalize(raw.at[1], 2)
    project_kv(3)
    project_kv(2)
    kv_out(1)
    twin_arrivals(q_weights, cq_recv)
    twin_start(near_parts, co_send, co_recv)
    for i in (0, 1):
        part = far.at[dp, chunks[i]]
        sent.append(
            send(wo.at[chunks[i], other_cols], part, cf_send.at[0, i], cf_recv.at[0, i], twin)
        )

    gain_rows = jnp.broadcast_to(gain_q, (HEAD, HEAD)).T[:, 0:1]

    def project_q(slot, c):
        cut = q_weights[...].reshape(WIDTH, 512)
        values = jnp.dot(normed[slot], cut, preferred_element_type=F32)
        for h in range(4):
            v = values[:, h * HEAD : (h + 1) * HEAD].T
            ms = jnp.mean(v * v, axis=0, keepdims=True)
            v = v * lax.rsqrt(ms + EPS) * gain_rows
            other = jnp.concatenate([v[32:64], v[0:32], v[96:128], v[64:96]], axis=0)
            q = v * cosines_t[slot] + other * sines_t[slot]
            q = q.astype(BF16).astype(F32) * (HEAD**-0.5 * LOG2E)
            coarse = q.astype(BF16)
            fine = (q - coarse.astype(F32)).astype(BF16)
            cols = pl.ds(pl.multiple_of(slot * KEYS + h * ROWS, ROWS), ROWS)
            qt[0:HEAD, cols] = coarse
            qt[HEAD : 2 * HEAD, cols] = fine
        return c

    lax.fori_loop(0, 2, project_q, 0)
    ring_events(near_ring, 1, (0,))
    lax.fori_loop(2, GROUP, project_q, 0)
    ring_events(near_ring, 1, (1,))

    def far_out(step, i):
        for way in (0, 1):
            if step < 4 or i == way:
                source, slot = source_of(way, step), slot_of(way, step)
                sent.append(
                    send(
                        near.at[source, chunks[i], pl.ds(SHARED, FAR)],
                        far.at[source, chunks[i]],
                        far_send.at[slot, i],
                        far_recv.at[slot, i],
                        (nxt, prv)[i],
                    )
                )

    def far_pass(step, i):
        for way in (0, 1):
            if step < 4 or i == way:
                slot = slot_of(way, step)
                part = far.at[source_of(way, step), chunks[i]]
                arrival(part, far_recv.at[slot, i])
                sent.append(send(part, part, cf_send.at[slot, i], cf_recv.at[slot, i], twin))

    ones = jnp.ones((ONES, KEYS), BF16)
    for d in range(GROUP):
        vbuf[d, HEAD : HEAD + ONES, :] = ones
    row_max[...] = jnp.full_like(row_max, -1e30)
    acc[...] = jnp.zeros_like(acc)
    size = 256

    def attend(nt, sn, topn, next_keys, ct, sc, topc, keys):
        if sc is not None:
            cols = span(ct, BQ)
            old = row_max[:, cols]
            new = jnp.maximum(old, jnp.max(topc[...], axis=0, keepdims=True))
            row_max[:, cols] = new
            decay = jnp.exp2(old - new)
        top, total = None, None
        for c in range(KEYS // size):
            part = pl.ds(c * size, size)
            if sn is not None:
                d, begin = next_keys[c]
                k = kbuf[d, pl.ds(begin, size), :]
                s = jnp.dot(
                    jnp.concatenate([k, k], axis=1),
                    qt[:, span(nt, BQ)],
                    preferred_element_type=F32,
                )
                sn[part, :] = s
                most = jnp.max(s.reshape(size // 8, 8, BQ), axis=0)
                top = most if top is None else jnp.maximum(top, most)
            if sc is not None:
                d, begin = keys[c]
                p = jnp.exp2(sc[part, :] - new).astype(BF16)
                v = jnp.dot(
                    vbuf[d, :, pl.ds(begin, size)], p, preferred_element_type=F32
                )
                total = v if total is None else total + v
        if sn is not None:
            topn[...] = top
        if sc is not None:
            acc[:, cols] = acc[:, cols] * decay + total

    def attend_block(keys, next_keys, next_tile, middle, late):
        def pair(i, c):
            t = i * 2
            attend(t + 1, s1, top1, keys, t, s0, top0, keys)
            attend(t + 2, s0, top0, keys, t + 1, s1, top1, keys)
            return c

        lax.fori_loop(0, TILES // 4, pair, 0)
        middle()
        lax.fori_loop(TILES // 4, TILES // 2 - 1, pair, 0)
        late()
        t = TILES - 2
        attend(t + 1, s1, top1, keys, t, s0, top0, keys)
        attend(next_tile, s0, top0, next_keys, t + 1, s1, top1, keys)

    quarters = [i * size for i in range(KEYS // size)]
    own = [(0, i) for i in quarters]
    firsts = [(3, i) for i in quarters[:2]] + [(1, i) for i in quarters[:2]]
    seconds = [(3, i) for i in quarters[2:]] + [(1, i) for i in quarters[2:]]
    opposite = [(2, i) for i in quarters]
    slots = (2, 1, 3, 0)

    attend(0, s0, top0, own, None, None, None, None)

    def middle0():
        ring_events(near_ring, 2, (0,))

    def late0():
        kv_pass(0)
        kv_arrival(3, 1, 0)
        kv_arrival(1, 0, 0)
        far_out(1, 0)
        far_out(1, 1)

    attend_block(own, firsts, 0, middle0, late0)

    def middle1():
        ring_events(near_ring, 2, (1,))

    def late1():
        ring_events(near_ring, 3, (0,))
        kv_pass(1)
        kv_arrival(3, 1, 1)
        kv_arrival(1, 0, 1)
        far_out(2, 0)
        far_out(2, 1)

    attend_block(firsts, seconds, 0, middle1, late1)

    def middle2():
        ring_events(near_ring, 3, (1,))
        far_pass(1, 0)
        far_pass(1, 1)
        far_out(3, 0)

    def late2():
        for half in (0, 1):
            kv_arrival(2, 0, half)
            kv_arrival(2, 1, half)
        far_out(3, 1)

    attend_block(seconds, opposite, 2 * slots[0], middle2, late2)

    ring_events(near_ring, 4)
    far_out(4, 0)
    far_out(4, 1)
    far_pass(2, 0)
    far_pass(2, 1)

    def hand_back(slot):
        for h in range(4):
            cols = pl.ds(slot * KEYS + h * ROWS, ROWS)
            scaled = acc[0:HEAD, cols] / acc[HEAD : HEAD + 1, cols]
            attended[slot, :, h * HEAD : (h + 1) * HEAD] = scaled.T.astype(BF16)
        if slot:
            sent.append(
                send(
                    attended.at[slot],
                    returned.at[group],
                    ret_send.at[slot - 1],
                    ret_recv.at[slot - 1],
                    {"sp": member(slot)},
                )
            )
        else:
            returned[group] = attended[0]

    for n, slot in enumerate(slots):
        t = 2 * slot
        after = 2 * slots[n + 1] if n < 3 else None
        attend(t + 1, s1, top1, opposite, t, s0, top0, opposite)
        attend(after, None if after is None else s0, top0, opposite, t + 1, s1, top1, opposite)
        hand_back(slot)
        if n == 1:
            far_pass(3, 0)
            far_pass(3, 1)
    for i in (0, 1):
        far_pass(4, i)
    for slot in (1, 2, 3):
        arrival(returned.at[(group + 4 - slot) % 4], ret_recv.at[slot - 1])
    twin_arrivals(near, co_recv)

    def project_out(columns):
        total = None
        for g in range(4):
            w = [
                buf[g * 4 : (g + 1) * 4, :, begin : begin + width].reshape(512, width)
                for buf, begin, width in columns
            ]
            w = w[0] if len(w) == 1 else jnp.concatenate(w, axis=1)
            d = jnp.dot(returned[g], w, preferred_element_type=F32)
            total = d if total is None else total + d
        return total, jnp.sum(total * total, axis=-1, keepdims=True)

    def side_of(which, begin, width):
        return pl.ds(pl.multiple_of(SHARED + which * FAR + begin, 256), width)

    total, squares = project_out([(near, 0, 512)])
    projected[:, 0:SHARED] = total
    total, more = project_out([(near, SHARED, 512)])
    projected[:, side_of(side, 0, 512)] = total
    squares = squares + more
    twin_arrivals(far, cf_recv)
    total, more = project_out([(far, 0, 512)])
    projected[:, side_of(1 - side, 0, 512)] = total
    squares = squares + more
    total, more = project_out([(near, SHARED + 512, 256), (far, 512, 256)])
    projected[:, side_of(side, 512, 256)] = total[:, 0:256]
    projected[:, side_of(1 - side, 512, 256)] = total[:, 256:512]
    squares = squares + more
    scale = lax.rsqrt(squares * (1.0 / WIDTH) + EPS)
    out[0] = (projected[...] * scale * out_gain[...]).astype(BF16)

    for copy in sent:
        copy.wait_send()


def on_device(tokens, in_gain, wq, wk, wv, q_gain, k_gain, wo, out_gain):
    vmem = pl.BlockSpec(memory_space=pltpu.VMEM)
    hbm = pl.BlockSpec(memory_space=pl.ANY)
    dma = pltpu.SemaphoreType.DMA
    ring, other_core = dma((2, 4, 2)), dma((Z, 2))
    return pl.pallas_call(
        kernel,
        out_shape=jax.ShapeDtypeStruct((1, ROWS, WIDTH), BF16),
        in_specs=[hbm] * 9,
        out_specs=vmem,
        scratch_shapes=[
            pltpu.VMEM((1, WIDTH), F32),
            pltpu.VMEM((1, HEAD), F32),
            pltpu.VMEM((1, HEAD), F32),
            pltpu.VMEM((1, WIDTH), F32),
            pltpu.VMEM((ROWS, WIDTH), BF16),
            pltpu.VMEM(wq.shape, BF16),
            pltpu.VMEM(wk.shape, BF16),
            pltpu.VMEM(wv.shape, BF16),
            pltpu.VMEM(wo.shape, BF16),
            pltpu.VMEM((3, ROWS, WIDTH), BF16),
            pltpu.VMEM((GROUP, ROWS, WIDTH), BF16),
            pltpu.VMEM((2 * Z, SHARD, 2 * HEAD), BF16),
            pltpu.VMEM((2 * Z, SHARD, 512), BF16),
            pltpu.VMEM((2 * Z, SHARD, NEAR), BF16),
            pltpu.VMEM((2 * Z, SHARD, FAR), BF16),
            pltpu.VMEM((GROUP, ROWS, HEAD), F32),
            pltpu.VMEM((GROUP, ROWS, HEAD), F32),
            pltpu.VMEM((GROUP, HEAD, ROWS), F32),
            pltpu.VMEM((GROUP, HEAD, ROWS), F32),
            pltpu.VMEM((2 * HEAD, KEYS * GROUP), BF16),
            pltpu.VMEM((GROUP, KEYS, HEAD), BF16),
            pltpu.VMEM((GROUP, HEAD + ONES, KEYS), BF16),
            pltpu.VMEM((KEYS, BQ), F32),
            pltpu.VMEM((KEYS, BQ), F32),
            pltpu.VMEM((8, BQ), F32),
            pltpu.VMEM((8, BQ), F32),
            pltpu.VMEM((1, KEYS * GROUP), F32),
            pltpu.VMEM((HEAD + ONES, KEYS * GROUP), F32),
            pltpu.VMEM((GROUP, ROWS, 512), BF16),
            pltpu.VMEM((GROUP, ROWS, 512), BF16),
            pltpu.VMEM((ROWS, WIDTH), F32),
            dma((9,)),
            dma((6,)),
            dma((6,)),
            *([ring, ring, other_core, other_core] * 3),
            *([other_core] * 4),
            dma((12,)),
            dma((12,)),
            dma((3,)),
            dma((3,)),
        ],
        compiler_params=pltpu.CompilerParams(
            collective_id=0, has_side_effects=True, vmem_limit_bytes=60 * 2**20
        ),
        name="grouped_attention",
    )(
        tokens,
        in_gain.reshape(1, WIDTH),
        wq,
        wk,
        wv,
        q_gain.reshape(1, HEAD),
        k_gain.reshape(1, HEAD),
        wo,
        out_gain.reshape(1, WIDTH),
    )


def solution(mesh):
    placed = (
        P("dp", "sp", None),
        P(),
        P("dp", None),
        P("dp", None),
        P("dp", None),
        P(),
        P(),
        P("dp", None),
        P(),
    )
    return jax.shard_map(
        on_device, mesh=mesh, in_specs=placed, out_specs=P("dp", "sp", None), check_vma=False
    )
```

```python
import jax
import jax.numpy as jnp
from jax import lax
from jax.experimental import pallas as pl
from jax.experimental.pallas import tpu as pltpu
from jax.sharding import PartitionSpec as P

MESH = pl.DeviceIdType.MESH
F32 = jnp.float32
BF16 = jnp.bfloat16

EPS = 1e-06
THETA = 10000.0
GRID_W = 64
HEAD = 128
WIDTH = 2048
ROWS = 256
GROUP = 4
KEYS = GROUP * ROWS
Z = 8
SHARD = WIDTH // (2 * Z)
NEAR = 1280
SHARED = 512
FAR = 768
HALF = ROWS // 2
BQ = 512
TILES = KEYS * GROUP // BQ
ONES = 16
LOG2E = 1.4426950408889634


def span(index, size):
    return pl.ds(pl.multiple_of(index * size, size), size)


def kernel(
    tokens_in,
    in_gain_in,
    wq_in,
    wk_in,
    wv_in,
    q_gain_in,
    k_gain_in,
    wo_in,
    out_gain_in,
    out,
    in_gain,
    q_gain,
    k_gain,
    out_gain,
    tokens,
    wq,
    wk,
    wv,
    wo,
    raw,
    normed,
    kv_weights,
    q_weights,
    near,
    far,
    cosines,
    sines,
    cosines_t,
    sines_t,
    qt,
    kbuf,
    vbuf,
    s0,
    s1,
    top0,
    top1,
    row_max,
    acc,
    attended,
    returned,
    projected,
    mixed,
    in_sem,
    out_sem,
    ag_send,
    ag_recv,
    zk_send,
    zk_recv,
    ck_send,
    ck_recv,
    zq_send,
    zq_recv,
    cq_send,
    cq_recv,
    zo_send,
    zo_recv,
    co_send,
    co_recv,
    far_send,
    far_recv,
    cf_send,
    cf_recv,
    kv_send,
    kv_recv,
    ret_send,
    ret_recv,
):
    staged = []
    for i, (src, dst) in enumerate(
        (
            (tokens_in.at[0], tokens),
            (wk_in, wk),
            (wv_in, wv),
            (wq_in, wq),
            (wo_in, wo),
            (in_gain_in, in_gain),
            (q_gain_in, q_gain),
            (k_gain_in, k_gain),
            (out_gain_in, out_gain),
        )
    ):
        staged.append(pltpu.make_async_copy(src, dst, in_sem.at[i]))
        staged[-1].start()

    sp = lax.axis_index("sp")
    dp = lax.axis_index("dp")
    y, x = sp // 4, sp % 4
    z, core = dp // 2, dp % 2
    at = (1 - core) * y + core * x
    group = (y + x) % 4
    side = group % 2

    def member(step):
        to = (at + step) % 4
        return (1 - core) * (to * 4 + x) + core * (y * 4 + to)

    def diagonal(step):
        return ((y + 4 - step) % 4) * 4 + (x + step) % 4

    up = {"dp": ((z + 1) % Z) * 2 + core}
    down = {"dp": ((z + Z - 1) % Z) * 2 + core}
    twin = {"dp": z * 2 + 1 - core}
    peers = [{"sp": member(1)}, {"sp": member(3)}, {"sp": member(2)}]
    peers += [{"sp": diagonal(1)}, {"sp": diagonal(3)}, up, down, twin]

    barrier = pltpu.get_barrier_semaphore()
    for peer in peers:
        pl.semaphore_signal(barrier, inc=1, device_id=peer, device_id_type=MESH)
    for copy in staged[:4]:
        copy.wait()
    pl.semaphore_wait(barrier, len(peers))

    sent = []

    def send(src, dst, send_sem, recv_sem, to):
        copy = pltpu.make_async_remote_copy(
            src_ref=src,
            dst_ref=dst,
            send_sem=send_sem,
            recv_sem=recv_sem,
            device_id=to,
            device_id_type=MESH,
        )
        copy.start()
        return copy

    def send_parts(pairs, whole, send_sem, recv_sem, to):
        for src, dst in pairs:
            send(src, dst, send_sem, recv_sem, to)
        sent.append(
            pltpu.make_async_remote_copy(
                src_ref=whole,
                dst_ref=whole,
                send_sem=send_sem,
                recv_sem=recv_sem,
                device_id=to,
                device_id_type=MESH,
            )
        )

    def arrival(ref, sem):
        pltpu.make_async_copy(ref, ref, sem).wait()

    low, high = pl.ds(0, HALF), pl.ds(HALF, HALF)
    nxt, prv = {"sp": member(1)}, {"sp": member(3)}

    def token_send(src, slot, part, index, to):
        sent.append(
            send(src, raw.at[slot - 1, part], ag_send.at[index], ag_recv.at[index], to)
        )

    token_send(tokens.at[low], 3, low, 0, nxt)
    token_send(tokens.at[high], 1, high, 1, prv)
    token_send(tokens.at[high], 3, high, 2, nxt)
    token_send(tokens.at[low], 1, low, 3, prv)

    chunks = (pl.ds(0, SHARD // 2), pl.ds(SHARD // 2, SHARD // 2))
    q_cols = span(group, 512)
    kv_cols = span(group, HEAD)
    side_cols = pl.ds(pl.multiple_of(SHARED + side * FAR, 256), FAR)
    other_cols = pl.ds(pl.multiple_of(SHARED + (1 - side) * FAR, 256), FAR)

    def kv_parts(i):
        mine = kv_weights.at[dp, chunks[i]]
        pairs = [
            (wk.at[chunks[i], kv_cols], mine.at[:, pl.ds(0, HEAD)]),
            (wv.at[chunks[i], kv_cols], mine.at[:, pl.ds(HEAD, HEAD)]),
        ]
        return pairs, mine

    def q_parts(i):
        mine = q_weights.at[dp, chunks[i]]
        return [(wq.at[chunks[i], q_cols], mine)], mine

    def near_parts(i):
        mine = near.at[dp, chunks[i]]
        pairs = [
            (wo.at[chunks[i], pl.ds(0, SHARED)], mine.at[:, pl.ds(0, SHARED)]),
            (wo.at[chunks[i], side_cols], mine.at[:, pl.ds(SHARED, FAR)]),
        ]
        return pairs, mine

    def ring_start(parts, zs, zr):
        for turn in (0, 1):
            for way, to in ((0, up), (1, down)):
                i = turn ^ way
                send_parts(*parts(i), zs.at[way, 0, i], zr.at[way, 0, i], to)

    def twin_start(parts, cs, cr):
        for i in (0, 1):
            send_parts(*parts(i), cs.at[0, i], cr.at[0, i], twin)

    def source_of(way, step):
        return (((z + Z - step) % Z) if way == 0 else ((z + step) % Z)) * 2 + core

    def slot_of(way, step):
        return step if way == 0 else Z - step

    def ring_event(buf, zs, zr, cs, cr, way, step, i):
        part = buf.at[source_of(way, step), chunks[i]]
        arrival(part, zr.at[way, step - 1, i])
        if step < 3 or (step == 3 and i == way):
            sent.append(
                send(part, part, zs.at[way, step, i], zr.at[way, step, i], (up, down)[way])
            )
        slot = slot_of(way, step)
        sent.append(send(part, part, cs.at[slot, i], cr.at[slot, i], twin))

    def ring_events(ring, step, turns=(0, 1)):
        for turn in turns:
            for way in (0, 1):
                if step < 4 or turn == 0:
                    ring_event(*ring, way, step, turn ^ way)

    def twin_arrivals(buf, cr, first=0):
        for slot in range(first, Z):
            source = ((z + Z - slot) % Z) * 2 + 1 - core
            for i in (0, 1):
                arrival(buf.at[source, chunks[i]], cr.at[slot, i])

    kv_ring = (kv_weights, zk_send, zk_recv, ck_send, ck_recv)
    q_ring = (q_weights, zq_send, zq_recv, cq_send, cq_recv)
    near_ring = (near, zo_send, zo_recv, co_send, co_recv)

    ring_start(kv_parts, zk_send, zk_recv)
    ring_start(q_parts, zq_send, zq_recv)
    twin_start(kv_parts, ck_send, ck_recv)
    twin_start(q_parts, cq_send, cq_recv)

    for copy in staged[4:]:
        copy.wait()
    kv_weights[dp, :, 0:HEAD] = wk[:, kv_cols]
    kv_weights[dp, :, HEAD : 2 * HEAD] = wv[:, kv_cols]
    q_weights[dp] = wq[:, q_cols]
    near[dp, :, 0:SHARED] = wo[:, 0:SHARED]
    near[dp, :, SHARED:NEAR] = wo[:, side_cols]
    far[dp] = wo[:, other_cols]

    gain_in = in_gain[...]

    def normalize(src, slot):
        def rows(i, c):
            part = pl.ds(pl.multiple_of(i * 32, 32), 32)
            v = src[part, :].astype(F32)
            ms = jnp.mean(v * v, axis=-1, keepdims=True)
            normed[slot, part, :] = (v * lax.rsqrt(ms + EPS) * gain_in).astype(BF16)
            return c

        lax.fori_loop(0, ROWS // 32, rows, 0)

    def angles(slot, c):
        row = lax.broadcasted_iota(jnp.int32, (ROWS, HEAD), 0)
        lane = lax.broadcasted_iota(jnp.int32, (ROWS, HEAD), 1)
        power = (lane % 32).astype(F32) * (1.0 / 32.0)
        freq = jnp.exp(power * (-9.210340371976184))
        grid_row = member(slot) * (ROWS // GRID_W) + row // GRID_W
        place = jnp.where(lane < 64, grid_row, row % GRID_W).astype(F32)
        angle = place * freq
        cosine = jnp.cos(angle)
        sine = jnp.sin(angle)
        sine = jnp.where(lane % 64 < 32, -sine, sine)
        cosines[slot] = cosine
        sines[slot] = sine
        cosines_t[slot] = cosine.T
        sines_t[slot] = sine.T
        return c

    normalize(tokens, 0)
    ring_events(kv_ring, 1)
    ring_events(q_ring, 1)
    ring_events(kv_ring, 2)
    arrival(raw.at[2, low], ag_recv.at[0])
    token_send(raw.at[2, low], 2, low, 4, nxt)
    arrival(raw.at[0, high], ag_recv.at[1])
    token_send(raw.at[0, high], 2, high, 5, prv)
    ring_events(q_ring, 2)
    lax.fori_loop(0, GROUP, angles, 0)
    ring_events(kv_ring, 3)
    ring_events(q_ring, 3)
    arrival(raw.at[2, high], ag_recv.at[2])
    arrival(raw.at[0, low], ag_recv.at[3])
    normalize(raw.at[0], 1)
    ring_events(kv_ring, 4)
    normalize(raw.at[2], 3)
    ring_events(q_ring, 4)
    ring_start(near_parts, zo_send, zo_recv)
    twin_arrivals(kv_weights, ck_recv)

    gain_q, gain_k = q_gain[...], k_gain[...]
    lane_of = lax.broadcasted_iota(jnp.int32, (ROWS, HEAD), 1)
    first = lane_of % 64 < 32

    def finish(v, gain, slot):
        ms = jnp.mean(v * v, axis=-1, keepdims=True)
        v = v * lax.rsqrt(ms + EPS) * gain
        other = jnp.where(first, pltpu.roll(v, HEAD - 32, 1), pltpu.roll(v, 32, 1))
        return v * cosines[slot] + other * sines[slot]

    def project_kv(slot):
        cut = kv_weights[...].reshape(WIDTH, 2 * HEAD)
        values = jnp.dot(normed[slot], cut, preferred_element_type=F32)
        rows = pl.ds(slot * ROWS, ROWS)
        kbuf[0, rows, :] = finish(values[:, 0:HEAD], gain_k, slot).astype(BF16)
        vbuf[0, 0:HEAD, rows] = values[:, HEAD : 2 * HEAD].T.astype(BF16)

    def kv_part(d, what, half):
        part = pl.ds(half * KEYS // 2, KEYS // 2)
        return kbuf.at[d, part] if what == 0 else vbuf.at[d, pl.ds(0, HEAD), part]

    def kv_index(d, what, half):
        return (d - 1) * 4 + what * 2 + half

    def kv_send_to(src, slot, what, half, to):
        index = kv_index(slot, what, half)
        sent.append(
            send(
                kv_part(src, what, half),
                kv_part(slot, what, half),
                kv_send.at[index],
                kv_recv.at[index],
                {"sp": diagonal(to)},
            )
        )

    def kv_arrival(slot, what, half):
        arrival(kv_part(slot, what, half), kv_recv.at[kv_index(slot, what, half)])

    def kv_out(half):
        kv_send_to(0, 3, 0, half, 1)
        kv_send_to(0, 1, 1, half, 3)
        kv_send_to(0, 3, 1, half, 1)
        kv_send_to(0, 1, 0, half, 3)

    def kv_pass(half):
        kv_arrival(3, 0, half)
        kv_send_to(3, 2, 0, half, 1)
        kv_arrival(1, 1, half)
        kv_send_to(1, 2, 1, half, 3)

    project_kv(0)
    project_kv(1)
    kv_out(0)
    arrival(raw.at[1, low], ag_recv.at[4])
    arrival(raw.at[1, high], ag_recv.at[5])
    normalize(raw.at[1], 2)
    project_kv(3)
    project_kv(2)
    kv_out(1)
    twin_arrivals(q_weights, cq_recv)
    twin_start(near_parts, co_send, co_recv)
    for i in (0, 1):
        part = far.at[dp, chunks[i]]
        sent.append(
            send(wo.at[chunks[i], other_cols], part, cf_send.at[0, i], cf_recv.at[0, i], twin)
        )

    gain_rows = jnp.broadcast_to(gain_q, (HEAD, HEAD)).T[:, 0:1]

    def project_q(slot, c):
        cut = q_weights[...].reshape(WIDTH, 512)
        values = jnp.dot(normed[slot], cut, preferred_element_type=F32)
        for h in range(4):
            v = values[:, h * HEAD : (h + 1) * HEAD].T
            ms = jnp.mean(v * v, axis=0, keepdims=True)
            v = v * lax.rsqrt(ms + EPS) * gain_rows
            other = jnp.concatenate([v[32:64], v[0:32], v[96:128], v[64:96]], axis=0)
            q = v * cosines_t[slot] + other * sines_t[slot]
            q = q.astype(BF16).astype(F32) * (HEAD**-0.5 * LOG2E)
            coarse = q.astype(BF16)
            fine = (q - coarse.astype(F32)).astype(BF16)
            cols = pl.ds(pl.multiple_of(slot * KEYS + h * ROWS, ROWS), ROWS)
            qt[0:HEAD, cols] = coarse
            qt[HEAD : 2 * HEAD, cols] = fine
        return c

    lax.fori_loop(0, 2, project_q, 0)
    ring_events(near_ring, 1, (0,))
    lax.fori_loop(2, GROUP, project_q, 0)
    ring_events(near_ring, 1, (1,))

    def far_out(step, i):
        for way in (0, 1):
            if step < 4 or i == way:
                source, slot = source_of(way, step), slot_of(way, step)
                sent.append(
                    send(
                        near.at[source, chunks[i], pl.ds(SHARED, FAR)],
                        far.at[source, chunks[i]],
                        far_send.at[slot, i],
                        far_recv.at[slot, i],
                        (nxt, prv)[i],
                    )
                )

    def far_pass(step, i):
        for way in (0, 1):
            if step < 4 or i == way:
                slot = slot_of(way, step)
                part = far.at[source_of(way, step), chunks[i]]
                arrival(part, far_recv.at[slot, i])
                sent.append(send(part, part, cf_send.at[slot, i], cf_recv.at[slot, i], twin))

    ones = jnp.ones((ONES, KEYS), BF16)
    for d in range(GROUP):
        vbuf[d, HEAD : HEAD + ONES, :] = ones
    row_max[...] = jnp.full_like(row_max, -1e30)
    acc[...] = jnp.zeros_like(acc)
    size = 512

    def attend(nt, sn, topn, next_keys, ct, sc, topc, keys):
        if sc is not None:
            cols = span(ct, BQ)
            old = row_max[:, cols]
            new = jnp.maximum(old, jnp.max(topc[...], axis=0, keepdims=True))
            row_max[:, cols] = new
            decay = jnp.exp2(old - new)
        top, total = None, None
        for c in range(KEYS // size):
            part = pl.ds(c * size, size)
            if sn is not None:
                d, begin = next_keys[c]
                k = kbuf[d, pl.ds(begin, size), :]
                s = jnp.dot(
                    jnp.concatenate([k, k], axis=1),
                    qt[:, span(nt, BQ)],
                    preferred_element_type=F32,
                )
                sn[part, :] = s
                most = jnp.max(s.reshape(size // 8, 8, BQ), axis=0)
                top = most if top is None else jnp.maximum(top, most)
            if sc is not None:
                d, begin = keys[c]
                p = jnp.exp2(sc[part, :] - new).astype(BF16)
                v = jnp.dot(
                    vbuf[d, :, pl.ds(begin, size)], p, preferred_element_type=F32
                )
                total = v if total is None else total + v
        if sn is not None:
            topn[...] = top
        if sc is not None:
            acc[:, cols] = acc[:, cols] * decay + total

    def hand_back(tile):
        slot, part = tile // 2, tile % 2
        two = pl.ds(part * 2 * HEAD, 2 * HEAD)
        for h in (0, 1):
            cols = pl.ds(tile * BQ + h * ROWS, ROWS)
            scaled = acc[0:HEAD, cols] / acc[HEAD : HEAD + 1, cols]
            begin = (part * 2 + h) * HEAD
            attended[slot, :, begin : begin + HEAD] = scaled.T.astype(BF16)
        if slot:
            sent.append(
                send(
                    attended.at[slot, :, two],
                    returned.at[group, :, two],
                    ret_send.at[slot - 1, part],
                    ret_recv.at[slot - 1, part],
                    {"sp": member(slot)},
                )
            )
        else:
            returned[group, :, two] = attended[0, :, two]

    blocks = (
        ((0, 0), (0, size)),
        ((3, 0), (1, 0)),
        ((3, size), (1, size)),
        ((2, 0), (2, size)),
    )
    steps = [(keys, tile) for keys in blocks[:3] for tile in range(TILES)]
    steps += [(blocks[3], tile) for tile in (4, 5, 2, 3, 6, 7, 0, 1)]
    buffers = ((s0, top0), (s1, top1))

    def keys_first():
        kv_pass(0)
        kv_arrival(3, 1, 0)
        kv_arrival(1, 0, 0)
        far_out(1, 0)
        far_out(1, 1)

    def keys_second():
        kv_pass(1)
        kv_arrival(3, 1, 1)
        kv_arrival(1, 0, 1)
        far_out(2, 0)
        far_out(2, 1)

    def keys_opposite():
        for half in (0, 1):
            kv_arrival(2, 0, half)
            kv_arrival(2, 1, half)

    def near_event(step, turns):
        ring_events(near_ring, step, turns)
        if step == 3 and turns == (1,):
            far_out(3, 0)
            far_out(3, 1)
            far_pass(1, 0)
            far_pass(1, 1)
        if step == 4:
            far_out(4, 0)
            far_out(4, 1)
            far_pass(2, 0)
            far_pass(2, 1)

    def far_third():
        far_pass(3, 0)
        far_pass(3, 1)

    events = {
        3: [lambda: near_event(2, (0,))],
        6: [keys_first],
        10: [lambda: near_event(2, (1,))],
        13: [lambda: near_event(3, (0,))],
        14: [keys_second],
        19: [lambda: near_event(3, (1,))],
        22: [keys_opposite],
        25: [lambda: near_event(4, (0,))],
        28: [far_third],
    }

    attend(steps[0][1], *buffers[0], steps[0][0], None, None, None, None)
    for n, (keys, tile) in enumerate(steps):
        now, later = buffers[n % 2], buffers[(n + 1) % 2]
        if n + 1 < len(steps):
            next_keys, next_tile = steps[n + 1]
            attend(next_tile, *later, next_keys, tile, *now, keys)
        else:
            attend(None, None, None, None, tile, *now, keys)
        if n >= 24:
            hand_back(tile)
        for event in events.get(n, ()):
            event()

    for i in (0, 1):
        far_pass(4, i)
    twin_arrivals(near, co_recv)

    def side_of(which, begin, width):
        return pl.ds(pl.multiple_of(SHARED + which * FAR + begin, 256), width)

    columns = (
        (((near, 0, 512),), ((0, pl.ds(0, 512)),)),
        (((near, SHARED, 512),), ((0, side_of(side, 0, 512)),)),
        (((far, 0, 512),), ((0, side_of(1 - side, 0, 512)),)),
        (
            ((near, SHARED + 512, 256), (far, 512, 256)),
            ((0, side_of(side, 512, 256)), (256, side_of(1 - side, 512, 256))),
        ),
    )

    def project_out(groups, lies):
        total = None
        for g in groups:
            w = [
                buf[span(g, 4), :, begin : begin + width].reshape(512, width)
                for buf, begin, width in lies
            ]
            w = w[0] if len(w) == 1 else jnp.concatenate(w, axis=1)
            d = jnp.dot(returned[g], w, preferred_element_type=F32)
            total = d if total is None else total + d
        return total

    def returns(slot):
        source = (group + 4 - slot) % 4
        for part in (0, 1):
            two = pl.ds(part * 2 * HEAD, 2 * HEAD)
            arrival(returned.at[source, :, two], ret_recv.at[slot - 1, part])

    returns(2)
    for n, (lies, places) in enumerate(columns):
        if n == 2:
            twin_arrivals(far, cf_recv)
        total = project_out((group, (group + 2) % 4), lies)
        for begin, place in places:
            projected[:, place] = total[:, begin : begin + place.size]
    returns(1)
    returns(3)
    squares = jnp.zeros((ROWS, 1), F32)
    for lies, places in columns:
        total = project_out(((group + 3) % 4, (group + 1) % 4), lies)
        for begin, place in places:
            value = projected[:, place] + total[:, begin : begin + place.size]
            projected[:, place] = value
            squares = squares + jnp.sum(value * value, axis=-1, keepdims=True)
    scale = lax.rsqrt(squares * (1.0 / WIDTH) + EPS)
    written = []
    for n in range(4):
        rows = slice(n * (ROWS // 4), (n + 1) * (ROWS // 4))
        mixed[rows, :] = (projected[rows, :] * scale[rows] * out_gain[...]).astype(BF16)
        written.append(
            pltpu.make_async_copy(mixed.at[pl.ds(n * (ROWS // 4), ROWS // 4)], out.at[0, pl.ds(n * (ROWS // 4), ROWS // 4)], out_sem.at[n])
        )
        written[-1].start()

    for copy in sent:
        copy.wait_send()
    for copy in written:
        copy.wait()


def on_device(tokens, in_gain, wq, wk, wv, q_gain, k_gain, wo, out_gain):
    hbm = pl.BlockSpec(memory_space=pl.ANY)
    dma = pltpu.SemaphoreType.DMA
    ring, other_core = dma((2, 4, 2)), dma((Z, 2))
    return pl.pallas_call(
        kernel,
        out_shape=jax.ShapeDtypeStruct((1, ROWS, WIDTH), BF16),
        in_specs=[hbm] * 9,
        out_specs=hbm,
        scratch_shapes=[
            pltpu.VMEM((1, WIDTH), F32),
            pltpu.VMEM((1, HEAD), F32),
            pltpu.VMEM((1, HEAD), F32),
            pltpu.VMEM((1, WIDTH), F32),
            pltpu.VMEM((ROWS, WIDTH), BF16),
            pltpu.VMEM(wq.shape, BF16),
            pltpu.VMEM(wk.shape, BF16),
            pltpu.VMEM(wv.shape, BF16),
            pltpu.VMEM(wo.shape, BF16),
            pltpu.VMEM((3, ROWS, WIDTH), BF16),
            pltpu.VMEM((GROUP, ROWS, WIDTH), BF16),
            pltpu.VMEM((2 * Z, SHARD, 2 * HEAD), BF16),
            pltpu.VMEM((2 * Z, SHARD, 512), BF16),
            pltpu.VMEM((2 * Z, SHARD, NEAR), BF16),
            pltpu.VMEM((2 * Z, SHARD, FAR), BF16),
            pltpu.VMEM((GROUP, ROWS, HEAD), F32),
            pltpu.VMEM((GROUP, ROWS, HEAD), F32),
            pltpu.VMEM((GROUP, HEAD, ROWS), F32),
            pltpu.VMEM((GROUP, HEAD, ROWS), F32),
            pltpu.VMEM((2 * HEAD, KEYS * GROUP), BF16),
            pltpu.VMEM((GROUP, KEYS, HEAD), BF16),
            pltpu.VMEM((GROUP, HEAD + ONES, KEYS), BF16),
            pltpu.VMEM((KEYS, BQ), F32),
            pltpu.VMEM((KEYS, BQ), F32),
            pltpu.VMEM((8, BQ), F32),
            pltpu.VMEM((8, BQ), F32),
            pltpu.VMEM((1, KEYS * GROUP), F32),
            pltpu.VMEM((HEAD + ONES, KEYS * GROUP), F32),
            pltpu.VMEM((GROUP, ROWS, 512), BF16),
            pltpu.VMEM((GROUP, ROWS, 512), BF16),
            pltpu.VMEM((ROWS, WIDTH), F32),
            pltpu.VMEM((ROWS, WIDTH), BF16),
            dma((9,)),
            dma((4,)),
            dma((6,)),
            dma((6,)),
            *([ring, ring, other_core, other_core] * 3),
            *([other_core] * 4),
            dma((12,)),
            dma((12,)),
            dma((3, 2)),
            dma((3, 2)),
        ],
        compiler_params=pltpu.CompilerParams(
            collective_id=0, has_side_effects=True, vmem_limit_bytes=60 * 2**20
        ),
        name="grouped_attention",
    )(
        tokens,
        in_gain.reshape(1, WIDTH),
        wq,
        wk,
        wv,
        q_gain.reshape(1, HEAD),
        k_gain.reshape(1, HEAD),
        wo,
        out_gain.reshape(1, WIDTH),
    )


def solution(mesh):
    placed = (
        P("dp", "sp", None),
        P(),
        P("dp", None),
        P("dp", None),
        P("dp", None),
        P(),
        P(),
        P("dp", None),
        P(),
    )
    return jax.shard_map(
        on_device, mesh=mesh, in_specs=placed, out_specs=P("dp", "sp", None), check_vma=False
    )
```

```python
import jax
import jax.numpy as jnp
from jax import lax
from jax.experimental import pallas as pl
from jax.experimental.pallas import tpu as pltpu
from jax.sharding import PartitionSpec as P

MESH = pl.DeviceIdType.MESH
F32 = jnp.float32
BF16 = jnp.bfloat16

EPS = 1e-06
THETA = 10000.0
GRID_W = 64
HEAD = 128
WIDTH = 2048
ROWS = 256
GROUP = 4
KEYS = GROUP * ROWS
Z = 8
SHARD = WIDTH // (2 * Z)
NEAR = 1280
SHARED = 512
FAR = 768
HALF = ROWS // 2
BQ = 512
TILES = KEYS * GROUP // BQ
ONES = 16
LOG2E = 1.4426950408889634


def span(index, size):
    return pl.ds(pl.multiple_of(index * size, size), size)


def kernel(
    tokens_in,
    in_gain_in,
    wq_in,
    wk_in,
    wv_in,
    q_gain_in,
    k_gain_in,
    wo_in,
    out_gain_in,
    out,
    in_gain,
    q_gain,
    k_gain,
    out_gain,
    tokens,
    wq,
    wk,
    wv,
    wo,
    raw,
    normed,
    kv_weights,
    q_weights,
    near,
    far,
    cosines,
    sines,
    cosines_t,
    sines_t,
    qt,
    kbuf,
    vbuf,
    s0,
    s1,
    top0,
    top1,
    row_max,
    acc,
    attended,
    returned,
    projected,
    mixed,
    in_sem,
    out_sem,
    ag_send,
    ag_recv,
    zk_send,
    zk_recv,
    ck_send,
    ck_recv,
    zq_send,
    zq_recv,
    cq_send,
    cq_recv,
    zo_send,
    zo_recv,
    co_send,
    co_recv,
    far_send,
    far_recv,
    cf_send,
    cf_recv,
    kv_send,
    kv_recv,
    ret_send,
    ret_recv,
):
    staged = []
    for i, (src, dst) in enumerate(
        (
            (tokens_in.at[0], tokens),
            (wk_in, wk),
            (wv_in, wv),
            (wq_in, wq),
            (wo_in, wo),
            (in_gain_in, in_gain),
            (q_gain_in, q_gain),
            (k_gain_in, k_gain),
            (out_gain_in, out_gain),
        )
    ):
        staged.append(pltpu.make_async_copy(src, dst, in_sem.at[i]))
        staged[-1].start()

    sp = lax.axis_index("sp")
    dp = lax.axis_index("dp")
    y, x = sp // 4, sp % 4
    z, core = dp // 2, dp % 2
    at = (1 - core) * y + core * x
    group = (y + x) % 4
    side = group % 2

    def member(step):
        to = (at + step) % 4
        return (1 - core) * (to * 4 + x) + core * (y * 4 + to)

    def diagonal(step):
        return ((y + 4 - step) % 4) * 4 + (x + step) % 4

    up = {"dp": ((z + 1) % Z) * 2 + core}
    down = {"dp": ((z + Z - 1) % Z) * 2 + core}
    twin = {"dp": z * 2 + 1 - core}
    peers = [{"sp": member(1)}, {"sp": member(3)}, {"sp": member(2)}]
    peers += [{"sp": diagonal(1)}, {"sp": diagonal(3)}, up, down, twin]

    barrier = pltpu.get_barrier_semaphore()
    for peer in peers:
        pl.semaphore_signal(barrier, inc=1, device_id=peer, device_id_type=MESH)
    for copy in staged[:4]:
        copy.wait()
    pl.semaphore_wait(barrier, len(peers))

    def send(src, dst, send_sem, recv_sem, to):
        copy = pltpu.make_async_remote_copy(
            src_ref=src,
            dst_ref=dst,
            send_sem=send_sem,
            recv_sem=recv_sem,
            device_id=to,
            device_id_type=MESH,
        )
        copy.start()

    def arrival(ref, sem):
        pltpu.make_async_copy(ref, ref, sem).wait()

    low, high = pl.ds(0, HALF), pl.ds(HALF, HALF)
    nxt, prv = {"sp": member(1)}, {"sp": member(3)}

    def token_send(src, slot, part, index, to):
        send(src, raw.at[slot - 1, part], ag_send, ag_recv.at[index], to)

    token_send(tokens.at[low], 3, low, 0, nxt)
    token_send(tokens.at[high], 1, high, 1, prv)
    token_send(tokens.at[high], 3, high, 2, nxt)
    token_send(tokens.at[low], 1, low, 3, prv)

    chunks = (pl.ds(0, SHARD // 2), pl.ds(SHARD // 2, SHARD // 2))
    q_cols = span(group, 512)
    kv_cols = span(group, HEAD)
    side_cols = pl.ds(pl.multiple_of(SHARED + side * FAR, 256), FAR)
    other_cols = pl.ds(pl.multiple_of(SHARED + (1 - side) * FAR, 256), FAR)

    def kv_parts(i):
        mine = kv_weights.at[dp, chunks[i]]
        return [
            (wk.at[chunks[i], kv_cols], mine.at[:, pl.ds(0, HEAD)]),
            (wv.at[chunks[i], kv_cols], mine.at[:, pl.ds(HEAD, HEAD)]),
        ]

    def q_parts(i):
        mine = q_weights.at[dp, chunks[i]]
        return [(wq.at[chunks[i], q_cols], mine)]

    def near_parts(i):
        mine = near.at[dp, chunks[i]]
        return [
            (wo.at[chunks[i], pl.ds(0, SHARED)], mine.at[:, pl.ds(0, SHARED)]),
            (wo.at[chunks[i], side_cols], mine.at[:, pl.ds(SHARED, FAR)]),
        ]

    def ring_start(parts, zs, zr):
        for turn in (0, 1):
            for way, to in ((0, up), (1, down)):
                i = turn ^ way
                for src, dst in parts(i):
                    send(src, dst, zs, zr.at[way, 0, i], to)

    def twin_start(parts, cs, cr):
        for i in (0, 1):
            for src, dst in parts(i):
                send(src, dst, cs, cr, twin)

    def source_of(way, step):
        return (((z + Z - step) % Z) if way == 0 else ((z + step) % Z)) * 2 + core

    def slot_of(way, step):
        return step if way == 0 else Z - step

    def ring_event(buf, zs, zr, cs, cr, way, step, i):
        part = buf.at[source_of(way, step), chunks[i]]
        arrival(part, zr.at[way, step - 1, i])
        if step < 3 or (step == 3 and i == way):
            send(part, part, zs, zr.at[way, step, i], (up, down)[way])
        send(part, part, cs, cr, twin)

    def ring_events(ring, step, turns=(0, 1)):
        for turn in turns:
            for way in (0, 1):
                if step < 4 or turn == 0:
                    ring_event(*ring, way, step, turn ^ way)

    def twin_arrivals(buf, cr):
        arrival(buf.at[pl.ds(0, Z)], cr)

    kv_ring = (kv_weights, zk_send, zk_recv, ck_send, ck_recv)
    q_ring = (q_weights, zq_send, zq_recv, cq_send, cq_recv)
    near_ring = (near, zo_send, zo_recv, co_send, co_recv)

    ring_start(kv_parts, zk_send, zk_recv)
    ring_start(q_parts, zq_send, zq_recv)
    twin_start(kv_parts, ck_send, ck_recv)
    twin_start(q_parts, cq_send, cq_recv)

    for copy in staged[4:]:
        copy.wait()
    kv_weights[dp, :, 0:HEAD] = wk[:, kv_cols]
    kv_weights[dp, :, HEAD : 2 * HEAD] = wv[:, kv_cols]
    q_weights[dp] = wq[:, q_cols]
    near[dp, :, 0:SHARED] = wo[:, 0:SHARED]
    near[dp, :, SHARED:NEAR] = wo[:, side_cols]
    far[dp] = wo[:, other_cols]

    gain_in = in_gain[...]

    def normalize(src, slot):
        def rows(i, c):
            part = pl.ds(pl.multiple_of(i * 32, 32), 32)
            v = src[part, :].astype(F32)
            ms = jnp.mean(v * v, axis=-1, keepdims=True)
            normed[slot, part, :] = (v * lax.rsqrt(ms + EPS) * gain_in).astype(BF16)
            return c

        lax.fori_loop(0, ROWS // 32, rows, 0, unroll=2)

    def angles(slot, c):
        row = lax.broadcasted_iota(jnp.int32, (ROWS, HEAD), 0)
        lane = lax.broadcasted_iota(jnp.int32, (ROWS, HEAD), 1)
        power = (lane % 32).astype(F32) * (1.0 / 32.0)
        freq = jnp.exp(power * (-9.210340371976184))
        grid_row = member(slot) * (ROWS // GRID_W) + row // GRID_W
        place = jnp.where(lane < 64, grid_row, row % GRID_W).astype(F32)
        angle = place * freq
        cosine = jnp.cos(angle)
        sine = jnp.sin(angle)
        sine = jnp.where(lane % 64 < 32, -sine, sine)
        cosines[slot] = cosine
        sines[slot] = sine
        cosines_t[slot] = cosine.T
        sines_t[slot] = sine.T
        return c

    normalize(tokens, 0)
    ring_events(kv_ring, 1)
    ring_events(q_ring, 1)
    ring_events(kv_ring, 2)
    arrival(raw.at[2, low], ag_recv.at[0])
    token_send(raw.at[2, low], 2, low, 4, nxt)
    arrival(raw.at[0, high], ag_recv.at[1])
    token_send(raw.at[0, high], 2, high, 5, prv)
    ring_events(q_ring, 2)
    lax.fori_loop(0, GROUP, angles, 0)
    ring_events(kv_ring, 3)
    ring_events(q_ring, 3)
    arrival(raw.at[2, high], ag_recv.at[2])
    arrival(raw.at[0, low], ag_recv.at[3])
    normalize(raw.at[0], 1)
    ring_events(kv_ring, 4)
    normalize(raw.at[2], 3)
    ring_events(q_ring, 4)
    ring_start(near_parts, zo_send, zo_recv)
    twin_arrivals(kv_weights, ck_recv)

    gain_q, gain_k = q_gain[...], k_gain[...]
    lane_of = lax.broadcasted_iota(jnp.int32, (ROWS, HEAD), 1)
    first = lane_of % 64 < 32

    def finish(v, gain, slot):
        ms = jnp.mean(v * v, axis=-1, keepdims=True)
        v = v * lax.rsqrt(ms + EPS) * gain
        other = jnp.where(first, pltpu.roll(v, HEAD - 32, 1), pltpu.roll(v, 32, 1))
        return v * cosines[slot] + other * sines[slot]

    def project_kv(slot):
        cut = kv_weights[...].reshape(WIDTH, 2 * HEAD)
        values = jnp.dot(normed[slot], cut, preferred_element_type=F32)
        rows = pl.ds(slot * ROWS, ROWS)
        kbuf[0, rows, :] = finish(values[:, 0:HEAD], gain_k, slot).astype(BF16)
        vbuf[0, 0:HEAD, rows] = values[:, HEAD : 2 * HEAD].T.astype(BF16)

    def kv_part(d, what, half):
        part = pl.ds(half * KEYS // 2, KEYS // 2)
        return kbuf.at[d, part] if what == 0 else vbuf.at[d, pl.ds(0, HEAD), part]

    def kv_index(d, what, half):
        return (d - 1) * 4 + what * 2 + half

    def kv_send_to(src, slot, what, half, to):
        index = kv_index(slot, what, half)
        send(
            kv_part(src, what, half),
            kv_part(slot, what, half),
            kv_send.at[what],
            kv_recv.at[index],
            {"sp": diagonal(to)},
        )

    def kv_arrival(slot, what, half):
        arrival(kv_part(slot, what, half), kv_recv.at[kv_index(slot, what, half)])

    def kv_out(half):
        kv_send_to(0, 3, 0, half, 1)
        kv_send_to(0, 1, 1, half, 3)
        kv_send_to(0, 3, 1, half, 1)
        kv_send_to(0, 1, 0, half, 3)

    def kv_pass(half):
        kv_arrival(3, 0, half)
        kv_send_to(3, 2, 0, half, 1)
        kv_arrival(1, 1, half)
        kv_send_to(1, 2, 1, half, 3)

    project_kv(0)
    project_kv(1)
    kv_out(0)
    arrival(raw.at[1, low], ag_recv.at[4])
    arrival(raw.at[1, high], ag_recv.at[5])
    normalize(raw.at[1], 2)
    project_kv(3)
    project_kv(2)
    kv_out(1)
    twin_arrivals(q_weights, cq_recv)
    twin_start(near_parts, co_send, co_recv)
    for i in (0, 1):
        send(wo.at[chunks[i], other_cols], far.at[dp, chunks[i]], cf_send, cf_recv, twin)

    gain_rows = jnp.broadcast_to(gain_q, (HEAD, HEAD)).T[:, 0:1]

    def project_q(slot):
        cut = q_weights[...].reshape(WIDTH, 512)
        values = jnp.dot(normed[slot], cut, preferred_element_type=F32)
        for h in range(4):
            v = values[:, h * HEAD : (h + 1) * HEAD].T
            ms = jnp.mean(v * v, axis=0, keepdims=True)
            v = v * lax.rsqrt(ms + EPS) * gain_rows
            other = jnp.concatenate([v[32:64], v[0:32], v[96:128], v[64:96]], axis=0)
            q = v * cosines_t[slot] + other * sines_t[slot]
            q = q.astype(BF16).astype(F32) * (HEAD**-0.5 * LOG2E)
            coarse = q.astype(BF16)
            fine = (q - coarse.astype(F32)).astype(BF16)
            cols = pl.ds(slot * KEYS + h * ROWS, ROWS)
            qt[0:HEAD, cols] = coarse
            qt[HEAD : 2 * HEAD, cols] = fine

    project_q(0)
    project_q(1)
    ring_events(near_ring, 1, (0,))
    project_q(2)
    project_q(3)
    ring_events(near_ring, 1, (1,))

    def far_out(step, i):
        for way in (0, 1):
            if step < 4 or i == way:
                source, slot = source_of(way, step), slot_of(way, step)
                send(
                    near.at[source, chunks[i], pl.ds(SHARED, FAR)],
                    far.at[source, chunks[i]],
                    far_send,
                    far_recv.at[slot, i],
                    (nxt, prv)[i],
                )

    def far_pass(step, i):
        for way in (0, 1):
            if step < 4 or i == way:
                slot = slot_of(way, step)
                part = far.at[source_of(way, step), chunks[i]]
                arrival(part, far_recv.at[slot, i])
                send(part, part, cf_send, cf_recv, twin)

    ones = jnp.ones((ONES, KEYS), BF16)
    for d in range(GROUP):
        vbuf[d, HEAD : HEAD + ONES, :] = ones
    row_max[...] = jnp.full_like(row_max, -1e30)
    acc[...] = jnp.zeros_like(acc)
    size = 512

    def attend(nt, sn, topn, next_keys, ct, sc, topc, keys):
        if sc is not None:
            cols = span(ct, BQ)
            old = row_max[:, cols]
            new = jnp.maximum(old, jnp.max(topc[...], axis=0, keepdims=True))
            row_max[:, cols] = new
            decay = jnp.exp2(old - new)
        top, total = None, None
        for c in range(KEYS // size):
            part = pl.ds(c * size, size)
            if sn is not None:
                d, begin = next_keys[c]
                k = kbuf[d, pl.ds(begin, size), :]
                s = jnp.dot(
                    jnp.concatenate([k, k], axis=1),
                    qt[:, span(nt, BQ)],
                    preferred_element_type=F32,
                )
                sn[part, :] = s
                most = jnp.max(s.reshape(size // 8, 8, BQ), axis=0)
                top = most if top is None else jnp.maximum(top, most)
            if sc is not None:
                d, begin = keys[c]
                p = jnp.exp2(sc[part, :] - new).astype(BF16)
                v = jnp.dot(
                    vbuf[d, :, pl.ds(begin, size)], p, preferred_element_type=F32
                )
                total = v if total is None else total + v
        if sn is not None:
            topn[...] = top
        if sc is not None:
            acc[:, cols] = acc[:, cols] * decay + total

    def hand_back(tile):
        slot, part = tile // 2, tile % 2
        two = pl.ds(part * 2 * HEAD, 2 * HEAD)
        for h in (0, 1):
            cols = pl.ds(tile * BQ + h * ROWS, ROWS)
            scaled = acc[0:HEAD, cols] / acc[HEAD : HEAD + 1, cols]
            begin = (part * 2 + h) * HEAD
            attended[slot, :, begin : begin + HEAD] = scaled.T.astype(BF16)
        if slot:
            send(
                attended.at[slot, :, two],
                returned.at[group, :, two],
                ret_send,
                ret_recv.at[slot - 1, part],
                {"sp": member(slot)},
            )
        else:
            returned[group, :, two] = attended[0, :, two]

    blocks = (
        ((0, 0), (0, size)),
        ((3, 0), (1, 0)),
        ((3, size), (1, size)),
        ((2, 0), (2, size)),
    )
    steps = [(keys, tile) for keys in blocks[:3] for tile in range(TILES)]
    steps += [(blocks[3], tile) for tile in (4, 5, 2, 3, 6, 7, 0, 1)]
    buffers = ((s0, top0), (s1, top1))

    def keys_first():
        kv_pass(0)
        kv_arrival(3, 1, 0)
        kv_arrival(1, 0, 0)
        far_out(1, 0)
        far_out(1, 1)

    def keys_second():
        kv_pass(1)
        kv_arrival(3, 1, 1)
        kv_arrival(1, 0, 1)
        far_out(2, 0)
        far_out(2, 1)

    def keys_opposite():
        for half in (0, 1):
            kv_arrival(2, 0, half)
            kv_arrival(2, 1, half)

    def near_event(step, turns):
        ring_events(near_ring, step, turns)
        if step == 3 and turns == (1,):
            far_out(3, 0)
            far_out(3, 1)
            far_pass(1, 0)
            far_pass(1, 1)
        if step == 4:
            far_out(4, 0)
            far_out(4, 1)
            far_pass(2, 0)
            far_pass(2, 1)

    def far_third():
        far_pass(3, 0)
        far_pass(3, 1)

    events = {
        4: [lambda: near_event(2, (0,))],
        6: [keys_first],
        10: [lambda: near_event(2, (1,))],
        13: [lambda: near_event(3, (0,))],
        14: [keys_second],
        19: [lambda: near_event(3, (1,))],
        22: [keys_opposite],
        24: [lambda: near_event(4, (0,))],
        28: [far_third],
    }

    attend(steps[0][1], *buffers[0], steps[0][0], None, None, None, None)
    for n, (keys, tile) in enumerate(steps):
        now, later = buffers[n % 2], buffers[(n + 1) % 2]
        if n + 1 < len(steps):
            next_keys, next_tile = steps[n + 1]
            attend(next_tile, *later, next_keys, tile, *now, keys)
        else:
            attend(None, None, None, None, tile, *now, keys)
        if n >= 24:
            hand_back(tile)
        for event in events.get(n, ()):
            event()

    for i in (0, 1):
        far_pass(4, i)
    twin_arrivals(near, co_recv)

    def side_of(which, begin, width):
        return pl.ds(pl.multiple_of(SHARED + which * FAR + begin, 256), width)

    columns = (
        (((near, 0, 512),), ((0, pl.ds(0, 512)),)),
        (((near, SHARED, 512),), ((0, side_of(side, 0, 512)),)),
        (((far, 0, 512),), ((0, side_of(1 - side, 0, 512)),)),
        (
            ((near, SHARED + 512, 256), (far, 512, 256)),
            ((0, side_of(side, 512, 256)), (256, side_of(1 - side, 512, 256))),
        ),
    )

    def project_out(groups, lies):
        total = None
        for g in groups:
            w = [
                buf[span(g, 4), :, begin : begin + width].reshape(512, width)
                for buf, begin, width in lies
            ]
            w = w[0] if len(w) == 1 else jnp.concatenate(w, axis=1)
            d = jnp.dot(returned[g], w, preferred_element_type=F32)
            total = d if total is None else total + d
        return total

    def returns(slot):
        source = (group + 4 - slot) % 4
        for part in (0, 1):
            two = pl.ds(part * 2 * HEAD, 2 * HEAD)
            arrival(returned.at[source, :, two], ret_recv.at[slot - 1, part])

    returns(2)
    for n, (lies, places) in enumerate(columns):
        if n == 2:
            twin_arrivals(far, cf_recv)
        total = project_out((group, (group + 2) % 4), lies)
        for begin, place in places:
            projected[:, place] = total[:, begin : begin + place.size]
    returns(1)
    returns(3)
    squares = jnp.zeros((ROWS, 1), F32)
    for lies, places in columns:
        total = project_out(((group + 3) % 4, (group + 1) % 4), lies)
        for begin, place in places:
            value = projected[:, place] + total[:, begin : begin + place.size]
            projected[:, place] = value
            squares = squares + jnp.sum(value * value, axis=-1, keepdims=True)
    scale = lax.rsqrt(squares * (1.0 / WIDTH) + EPS)
    written = []
    for n in range(4):
        rows = slice(n * (ROWS // 4), (n + 1) * (ROWS // 4))
        mixed[rows, :] = (projected[rows, :] * scale[rows] * out_gain[...]).astype(BF16)
        written.append(
            pltpu.make_async_copy(mixed.at[pl.ds(n * (ROWS // 4), ROWS // 4)], out.at[0, pl.ds(n * (ROWS // 4), ROWS // 4)], out_sem.at[n])
        )
        written[-1].start()

    ring_bytes, twin_bytes = pl.ds(0, Z - 1), pl.ds(0, Z)
    for buf, zs, _, cs, _ in (kv_ring, q_ring, near_ring):
        arrival(buf.at[ring_bytes], zs)
        arrival(buf.at[twin_bytes], cs)
    arrival(far.at[ring_bytes], far_send)
    arrival(far.at[twin_bytes], cf_send)
    arrival(raw, ag_send)
    arrival(kbuf.at[pl.ds(0, 3)], kv_send.at[0])
    arrival(vbuf.at[pl.ds(0, 3), pl.ds(0, HEAD)], kv_send.at[1])
    arrival(attended.at[pl.ds(0, 3)], ret_send)
    for copy in written:
        copy.wait()


def on_device(tokens, in_gain, wq, wk, wv, q_gain, k_gain, wo, out_gain):
    hbm = pl.BlockSpec(memory_space=pl.ANY)
    dma = pltpu.SemaphoreType.DMA
    one = dma(())
    ring = dma((2, 4, 2))
    return pl.pallas_call(
        kernel,
        out_shape=jax.ShapeDtypeStruct((1, ROWS, WIDTH), BF16),
        in_specs=[hbm] * 9,
        out_specs=hbm,
        scratch_shapes=[
            pltpu.VMEM((1, WIDTH), F32),
            pltpu.VMEM((1, HEAD), F32),
            pltpu.VMEM((1, HEAD), F32),
            pltpu.VMEM((1, WIDTH), F32),
            pltpu.VMEM((ROWS, WIDTH), BF16),
            pltpu.VMEM(wq.shape, BF16),
            pltpu.VMEM(wk.shape, BF16),
            pltpu.VMEM(wv.shape, BF16),
            pltpu.VMEM(wo.shape, BF16),
            pltpu.VMEM((3, ROWS, WIDTH), BF16),
            pltpu.VMEM((GROUP, ROWS, WIDTH), BF16),
            pltpu.VMEM((2 * Z, SHARD, 2 * HEAD), BF16),
            pltpu.VMEM((2 * Z, SHARD, 512), BF16),
            pltpu.VMEM((2 * Z, SHARD, NEAR), BF16),
            pltpu.VMEM((2 * Z, SHARD, FAR), BF16),
            pltpu.VMEM((GROUP, ROWS, HEAD), F32),
            pltpu.VMEM((GROUP, ROWS, HEAD), F32),
            pltpu.VMEM((GROUP, HEAD, ROWS), F32),
            pltpu.VMEM((GROUP, HEAD, ROWS), F32),
            pltpu.VMEM((2 * HEAD, KEYS * GROUP), BF16),
            pltpu.VMEM((GROUP, KEYS, HEAD), BF16),
            pltpu.VMEM((GROUP, HEAD + ONES, KEYS), BF16),
            pltpu.VMEM((KEYS, BQ), F32),
            pltpu.VMEM((KEYS, BQ), F32),
            pltpu.VMEM((8, BQ), F32),
            pltpu.VMEM((8, BQ), F32),
            pltpu.VMEM((1, KEYS * GROUP), F32),
            pltpu.VMEM((HEAD + ONES, KEYS * GROUP), F32),
            pltpu.VMEM((GROUP, ROWS, 512), BF16),
            pltpu.VMEM((GROUP, ROWS, 512), BF16),
            pltpu.VMEM((ROWS, WIDTH), F32),
            pltpu.VMEM((ROWS, WIDTH), BF16),
            dma((9,)),
            dma((4,)),
            one,
            dma((6,)),
            *([one, ring, one, one] * 3),
            one,
            dma((Z, 2)),
            one,
            one,
            dma((2,)),
            dma((12,)),
            one,
            dma((3, 2)),
        ],
        compiler_params=pltpu.CompilerParams(
            collective_id=0, has_side_effects=True, vmem_limit_bytes=60 * 2**20
        ),
        name="grouped_attention",
    )(
        tokens,
        in_gain.reshape(1, WIDTH),
        wq,
        wk,
        wv,
        q_gain.reshape(1, HEAD),
        k_gain.reshape(1, HEAD),
        wo,
        out_gain.reshape(1, WIDTH),
    )


def solution(mesh):
    placed = (
        P("dp", "sp", None),
        P(),
        P("dp", None),
        P("dp", None),
        P("dp", None),
        P(),
        P(),
        P("dp", None),
        P(),
    )
    return jax.shard_map(
        on_device, mesh=mesh, in_specs=placed, out_specs=P("dp", "sp", None), check_vma=False
    )
```

```python
import jax
import jax.numpy as jnp
from jax import lax
from jax.experimental import pallas as pl
from jax.experimental.pallas import tpu as pltpu
from jax.sharding import PartitionSpec as P

MESH = pl.DeviceIdType.MESH
F32 = jnp.float32
BF16 = jnp.bfloat16

EPS = 1e-06
THETA = 10000.0
GRID_W = 64
HEAD = 128
WIDTH = 2048
ROWS = 256
GROUP = 4
KEYS = GROUP * ROWS
Z = 8
SHARD = WIDTH // (2 * Z)
NEAR = 1280
SHARED = 512
FAR = 768
HALF = ROWS // 2
BQ = 512
TILES = KEYS * GROUP // BQ
ONES = 16
LOG2E = 1.4426950408889634


def span(index, size):
    return pl.ds(pl.multiple_of(index * size, size), size)


def kernel(
    tokens_in,
    in_gain_in,
    wq_in,
    wk_in,
    wv_in,
    q_gain_in,
    k_gain_in,
    wo_in,
    out_gain_in,
    out,
    in_gain,
    q_gain,
    k_gain,
    out_gain,
    tokens,
    wq,
    wk,
    wv,
    wo,
    raw,
    normed,
    kv_weights,
    q_weights,
    near,
    far,
    cosines,
    sines,
    cosines_t,
    sines_t,
    qt,
    kbuf,
    vbuf,
    s0,
    s1,
    top0,
    top1,
    row_max,
    acc,
    attended,
    returned,
    projected,
    mixed,
    in_sem,
    out_sem,
    ag_send,
    ag_recv,
    zk_send,
    zk_recv,
    ck_send,
    ck_recv,
    zq_send,
    zq_recv,
    cq_send,
    cq_recv,
    zo_send,
    zo_recv,
    co_send,
    co_recv,
    far_send,
    far_recv,
    cf_send,
    cf_recv,
    kv_send,
    kv_recv,
    ret_send,
    ret_recv,
):
    staged = []
    for i, (src, dst) in enumerate(
        (
            (tokens_in.at[0], tokens),
            (wk_in, wk),
            (wv_in, wv),
            (wq_in, wq),
            (wo_in, wo),
            (in_gain_in, in_gain),
            (q_gain_in, q_gain),
            (k_gain_in, k_gain),
            (out_gain_in, out_gain),
        )
    ):
        staged.append(pltpu.make_async_copy(src, dst, in_sem.at[i]))
        staged[-1].start()

    sp = lax.axis_index("sp")
    dp = lax.axis_index("dp")
    y, x = sp // 4, sp % 4
    z, core = dp // 2, dp % 2
    at = (1 - core) * y + core * x
    group = (y + x) % 4
    side = group % 2

    def member(step):
        to = (at + step) % 4
        return (1 - core) * (to * 4 + x) + core * (y * 4 + to)

    def diagonal(step):
        return ((y + 4 - step) % 4) * 4 + (x + step) % 4

    up = {"dp": ((z + 1) % Z) * 2 + core}
    down = {"dp": ((z + Z - 1) % Z) * 2 + core}
    twin = {"dp": z * 2 + 1 - core}
    peers = [{"sp": member(1)}, {"sp": member(3)}, {"sp": member(2)}]
    peers += [{"sp": diagonal(1)}, {"sp": diagonal(3)}, up, down, twin]

    barrier = pltpu.get_barrier_semaphore()
    for peer in peers:
        pl.semaphore_signal(barrier, inc=1, device_id=peer, device_id_type=MESH)
    for copy in staged[:4]:
        copy.wait()
    pl.semaphore_wait(barrier, len(peers))

    def send(src, dst, send_sem, recv_sem, to):
        copy = pltpu.make_async_remote_copy(
            src_ref=src,
            dst_ref=dst,
            send_sem=send_sem,
            recv_sem=recv_sem,
            device_id=to,
            device_id_type=MESH,
        )
        copy.start()

    def arrival(ref, sem):
        pltpu.make_async_copy(ref, ref, sem).wait()

    low, high = pl.ds(0, HALF), pl.ds(HALF, HALF)
    nxt, prv = {"sp": member(1)}, {"sp": member(3)}

    def token_send(src, slot, part, index, to):
        send(src, raw.at[slot - 1, part], ag_send, ag_recv.at[index], to)

    token_send(tokens.at[low], 3, low, 0, nxt)
    token_send(tokens.at[high], 1, high, 1, prv)
    token_send(tokens.at[high], 3, high, 2, nxt)
    token_send(tokens.at[low], 1, low, 3, prv)

    chunks = (pl.ds(0, SHARD // 2), pl.ds(SHARD // 2, SHARD // 2))
    q_cols = span(group, 512)
    kv_cols = span(group, HEAD)
    side_cols = pl.ds(pl.multiple_of(SHARED + side * FAR, 256), FAR)
    other_cols = pl.ds(pl.multiple_of(SHARED + (1 - side) * FAR, 256), FAR)

    def kv_parts(i):
        mine = kv_weights.at[dp, chunks[i]]
        return [
            (wk.at[chunks[i], kv_cols], mine.at[:, pl.ds(0, HEAD)]),
            (wv.at[chunks[i], kv_cols], mine.at[:, pl.ds(HEAD, HEAD)]),
        ]

    def q_parts(i):
        mine = q_weights.at[dp, chunks[i]]
        return [(wq.at[chunks[i], q_cols], mine)]

    def near_parts(i):
        mine = near.at[dp, chunks[i]]
        return [
            (wo.at[chunks[i], pl.ds(0, SHARED)], mine.at[:, pl.ds(0, SHARED)]),
            (wo.at[chunks[i], side_cols], mine.at[:, pl.ds(SHARED, FAR)]),
        ]

    def ring_start(parts, zs, zr):
        for turn in (0, 1):
            for way, to in ((0, up), (1, down)):
                i = turn ^ way
                for src, dst in parts(i):
                    send(src, dst, zs, zr.at[way, 0, i], to)

    def twin_start(parts, cs, cr):
        for i in (0, 1):
            for src, dst in parts(i):
                send(src, dst, cs, cr, twin)

    def source_of(way, step):
        return (((z + Z - step) % Z) if way == 0 else ((z + step) % Z)) * 2 + core

    def slot_of(way, step):
        return step if way == 0 else Z - step

    def ring_event(buf, zs, zr, cs, cr, way, step, i):
        part = buf.at[source_of(way, step), chunks[i]]
        arrival(part, zr.at[way, step - 1, i])
        if step < 3 or (step == 3 and i == way):
            send(part, part, zs, zr.at[way, step, i], (up, down)[way])
        send(part, part, cs, cr, twin)

    def ring_events(ring, step, turns=(0, 1)):
        for turn in turns:
            for way in (0, 1):
                if step < 4 or turn == 0:
                    ring_event(*ring, way, step, turn ^ way)

    def twin_arrivals(buf, cr):
        arrival(buf.at[pl.ds(0, Z)], cr)

    kv_ring = (kv_weights, zk_send, zk_recv, ck_send, ck_recv)
    q_ring = (q_weights, zq_send, zq_recv, cq_send, cq_recv)
    near_ring = (near, zo_send, zo_recv, co_send, co_recv)

    ring_start(kv_parts, zk_send, zk_recv)
    ring_start(q_parts, zq_send, zq_recv)
    twin_start(kv_parts, ck_send, ck_recv)
    twin_start(q_parts, cq_send, cq_recv)

    for copy in staged[4:]:
        copy.wait()
    kv_weights[dp, :, 0:HEAD] = wk[:, kv_cols]
    kv_weights[dp, :, HEAD : 2 * HEAD] = wv[:, kv_cols]
    q_weights[dp] = wq[:, q_cols]
    near[dp, :, 0:SHARED] = wo[:, 0:SHARED]
    near[dp, :, SHARED:NEAR] = wo[:, side_cols]
    far[dp] = wo[:, other_cols]

    gain_in = in_gain[...]

    def normalize(src, slot):
        def rows(i, c):
            part = pl.ds(pl.multiple_of(i * 32, 32), 32)
            v = src[part, :].astype(F32)
            ms = jnp.mean(v * v, axis=-1, keepdims=True)
            normed[slot, part, :] = (v * lax.rsqrt(ms + EPS) * gain_in).astype(BF16)
            return c

        lax.fori_loop(0, ROWS // 32, rows, 0, unroll=2)

    def angles(slot, c):
        row = lax.broadcasted_iota(jnp.int32, (ROWS, HEAD), 0)
        lane = lax.broadcasted_iota(jnp.int32, (ROWS, HEAD), 1)
        power = (lane % 32).astype(F32) * (1.0 / 32.0)
        freq = jnp.exp(power * (-9.210340371976184))
        grid_row = member(slot) * (ROWS // GRID_W) + row // GRID_W
        place = jnp.where(lane < 64, grid_row, row % GRID_W).astype(F32)
        angle = place * freq
        cosine = jnp.cos(angle)
        sine = jnp.sin(angle)
        sine = jnp.where(lane % 64 < 32, -sine, sine)
        cosines[slot] = cosine
        sines[slot] = sine
        cosines_t[slot] = cosine.T
        sines_t[slot] = sine.T
        return c

    normalize(tokens, 0)
    lax.fori_loop(0, 2, angles, 0)
    ring_events(kv_ring, 1)
    lax.fori_loop(2, 3, angles, 0)
    ring_events(q_ring, 1)
    ring_events(kv_ring, 2)
    arrival(raw.at[2, low], ag_recv.at[0])
    token_send(raw.at[2, low], 2, low, 4, nxt)
    arrival(raw.at[0, high], ag_recv.at[1])
    token_send(raw.at[0, high], 2, high, 5, prv)
    lax.fori_loop(3, GROUP, angles, 0)
    ring_events(q_ring, 2)
    ring_events(kv_ring, 3)
    ring_events(q_ring, 3)
    arrival(raw.at[2, high], ag_recv.at[2])
    arrival(raw.at[0, low], ag_recv.at[3])
    normalize(raw.at[0], 1)
    ring_events(kv_ring, 4)
    normalize(raw.at[2], 3)
    ring_events(q_ring, 4)
    ring_start(near_parts, zo_send, zo_recv)
    twin_arrivals(kv_weights, ck_recv)

    gain_q, gain_k = q_gain[...], k_gain[...]
    lane_of = lax.broadcasted_iota(jnp.int32, (ROWS, HEAD), 1)
    first = lane_of % 64 < 32

    def finish(v, gain, slot):
        ms = jnp.mean(v * v, axis=-1, keepdims=True)
        v = v * lax.rsqrt(ms + EPS) * gain
        other = jnp.where(first, pltpu.roll(v, HEAD - 32, 1), pltpu.roll(v, 32, 1))
        return v * cosines[slot] + other * sines[slot]

    def project_kv(slot):
        cut = kv_weights[...].reshape(WIDTH, 2 * HEAD)
        values = jnp.dot(normed[slot], cut, preferred_element_type=F32)
        rows = pl.ds(slot * ROWS, ROWS)
        kbuf[0, rows, :] = finish(values[:, 0:HEAD], gain_k, slot).astype(BF16)
        vbuf[0, 0:HEAD, rows] = values[:, HEAD : 2 * HEAD].T.astype(BF16)

    def kv_part(d, what, half):
        part = pl.ds(half * KEYS // 2, KEYS // 2)
        return kbuf.at[d, part] if what == 0 else vbuf.at[d, pl.ds(0, HEAD), part]

    def kv_index(d, what, half):
        return (d - 1) * 4 + what * 2 + half

    def kv_send_to(src, slot, what, half, to):
        index = kv_index(slot, what, half)
        send(
            kv_part(src, what, half),
            kv_part(slot, what, half),
            kv_send.at[what],
            kv_recv.at[index],
            {"sp": diagonal(to)},
        )

    def kv_arrival(slot, what, half):
        arrival(kv_part(slot, what, half), kv_recv.at[kv_index(slot, what, half)])

    def kv_out(half):
        kv_send_to(0, 3, 0, half, 1)
        kv_send_to(0, 1, 1, half, 3)
        kv_send_to(0, 3, 1, half, 1)
        kv_send_to(0, 1, 0, half, 3)

    def kv_pass(half):
        kv_arrival(3, 0, half)
        kv_send_to(3, 2, 0, half, 1)
        kv_arrival(1, 1, half)
        kv_send_to(1, 2, 1, half, 3)

    project_kv(0)
    project_kv(1)
    kv_out(0)
    arrival(raw.at[1, low], ag_recv.at[4])
    arrival(raw.at[1, high], ag_recv.at[5])
    normalize(raw.at[1], 2)
    project_kv(3)
    project_kv(2)
    kv_out(1)
    twin_arrivals(q_weights, cq_recv)
    twin_start(near_parts, co_send, co_recv)
    for i in (0, 1):
        send(wo.at[chunks[i], other_cols], far.at[dp, chunks[i]], cf_send, cf_recv, twin)

    gain_rows = jnp.broadcast_to(gain_q, (HEAD, HEAD)).T[:, 0:1]

    def project_q(slot):
        cut = q_weights[...].reshape(WIDTH, 512)
        values = jnp.dot(normed[slot], cut, preferred_element_type=F32)
        for h in range(4):
            v = values[:, h * HEAD : (h + 1) * HEAD].T
            ms = jnp.mean(v * v, axis=0, keepdims=True)
            v = v * lax.rsqrt(ms + EPS) * gain_rows
            other = jnp.concatenate([v[32:64], v[0:32], v[96:128], v[64:96]], axis=0)
            q = v * cosines_t[slot] + other * sines_t[slot]
            q = q.astype(BF16).astype(F32) * (HEAD**-0.5 * LOG2E)
            coarse = q.astype(BF16)
            fine = (q - coarse.astype(F32)).astype(BF16)
            cols = pl.ds(slot * KEYS + h * ROWS, ROWS)
            qt[0:HEAD, cols] = coarse
            qt[HEAD : 2 * HEAD, cols] = fine

    project_q(0)
    project_q(1)
    project_q(2)
    ring_events(near_ring, 1, (0,))
    project_q(3)
    ring_events(near_ring, 1, (1,))

    def far_out(step, i):
        for way in (0, 1):
            if step < 4 or i == way:
                source, slot = source_of(way, step), slot_of(way, step)
                send(
                    near.at[source, chunks[i], pl.ds(SHARED, FAR)],
                    far.at[source, chunks[i]],
                    far_send,
                    far_recv.at[slot, i],
                    (nxt, prv)[i],
                )

    def far_pass(step, i):
        for way in (0, 1):
            if step < 4 or i == way:
                slot = slot_of(way, step)
                part = far.at[source_of(way, step), chunks[i]]
                arrival(part, far_recv.at[slot, i])
                send(part, part, cf_send, cf_recv, twin)

    ones = jnp.ones((ONES, KEYS), BF16)
    for d in range(GROUP):
        vbuf[d, HEAD : HEAD + ONES, :] = ones
    row_max[...] = jnp.full_like(row_max, -1e30)
    acc[...] = jnp.zeros_like(acc)
    size = 512

    def attend(nt, sn, topn, next_keys, ct, sc, topc, keys):
        if sc is not None:
            cols = span(ct, BQ)
            old = row_max[:, cols]
            new = jnp.maximum(old, jnp.max(topc[...], axis=0, keepdims=True))
            row_max[:, cols] = new
            decay = jnp.exp2(old - new)
        top, total = None, None
        for c in range(KEYS // size):
            part = pl.ds(c * size, size)
            if sn is not None:
                d, begin = next_keys[c]
                k = kbuf[d, pl.ds(begin, size), :]
                s = jnp.dot(
                    jnp.concatenate([k, k], axis=1),
                    qt[:, span(nt, BQ)],
                    preferred_element_type=F32,
                )
                sn[part, :] = s
                most = jnp.max(s.reshape(size // 8, 8, BQ), axis=0)
                top = most if top is None else jnp.maximum(top, most)
            if sc is not None:
                d, begin = keys[c]
                p = jnp.exp2(sc[part, :] - new).astype(BF16)
                v = jnp.dot(
                    vbuf[d, :, pl.ds(begin, size)], p, preferred_element_type=F32
                )
                total = v if total is None else total + v
        if sn is not None:
            topn[...] = top
        if sc is not None:
            acc[:, cols] = acc[:, cols] * decay + total

    def hand_back(tile):
        slot, part = tile // 2, tile % 2
        two = pl.ds(part * 2 * HEAD, 2 * HEAD)
        for h in (0, 1):
            cols = pl.ds(tile * BQ + h * ROWS, ROWS)
            scaled = acc[0:HEAD, cols] / acc[HEAD : HEAD + 1, cols]
            begin = (part * 2 + h) * HEAD
            attended[slot, :, begin : begin + HEAD] = scaled.T.astype(BF16)
        if slot:
            send(
                attended.at[slot, :, two],
                returned.at[group, :, two],
                ret_send,
                ret_recv.at[slot - 1, part],
                {"sp": member(slot)},
            )
        else:
            returned[group, :, two] = attended[0, :, two]

    blocks = (
        ((0, 0), (0, size)),
        ((3, 0), (1, 0)),
        ((3, size), (1, size)),
        ((2, 0), (2, size)),
    )
    steps = [(keys, tile) for keys in blocks[:3] for tile in range(TILES)]
    steps += [(blocks[3], tile) for tile in (4, 5, 2, 3, 6, 7, 0, 1)]
    buffers = ((s0, top0), (s1, top1))

    def keys_first():
        kv_pass(0)
        kv_arrival(3, 1, 0)
        kv_arrival(1, 0, 0)
        far_out(1, 0)
        far_out(1, 1)

    def keys_second():
        kv_pass(1)
        kv_arrival(3, 1, 1)
        kv_arrival(1, 0, 1)
        far_out(2, 0)
        far_out(2, 1)

    def keys_opposite():
        for half in (0, 1):
            kv_arrival(2, 0, half)
            kv_arrival(2, 1, half)

    def near_event(step, turns):
        ring_events(near_ring, step, turns)
        if step == 3 and turns == (1,):
            far_out(3, 0)
            far_out(3, 1)
            far_pass(1, 0)
            far_pass(1, 1)
        if step == 4:
            far_out(4, 0)
            far_out(4, 1)
            far_pass(2, 0)
            far_pass(2, 1)

    def far_third():
        far_pass(3, 0)
        far_pass(3, 1)

    events = {
        5: [lambda: near_event(2, (0,))],
        6: [keys_first],
        10: [lambda: near_event(2, (1,))],
        14: [keys_second, lambda: near_event(3, (0,))],
        19: [lambda: near_event(3, (1,))],
        22: [keys_opposite],
        24: [lambda: near_event(4, (0,))],
        28: [far_third],
    }

    attend(steps[0][1], *buffers[0], steps[0][0], None, None, None, None)
    for n, (keys, tile) in enumerate(steps):
        now, later = buffers[n % 2], buffers[(n + 1) % 2]
        if n + 1 < len(steps):
            next_keys, next_tile = steps[n + 1]
            attend(next_tile, *later, next_keys, tile, *now, keys)
        else:
            attend(None, None, None, None, tile, *now, keys)
        if n >= 24:
            hand_back(tile)
        for event in events.get(n, ()):
            event()

    for i in (0, 1):
        far_pass(4, i)
    twin_arrivals(near, co_recv)

    def side_of(which, begin, width):
        return pl.ds(pl.multiple_of(SHARED + which * FAR + begin, 256), width)

    columns = (
        (((near, 0, 512),), ((0, pl.ds(0, 512)),)),
        (((near, SHARED, 512),), ((0, side_of(side, 0, 512)),)),
        (((far, 0, 512),), ((0, side_of(1 - side, 0, 512)),)),
        (
            ((near, SHARED + 512, 256), (far, 512, 256)),
            ((0, side_of(side, 512, 256)), (256, side_of(1 - side, 512, 256))),
        ),
    )

    def project_out(groups, lies):
        total = None
        for g in groups:
            w = [
                buf[span(g, 4), :, begin : begin + width].reshape(512, width)
                for buf, begin, width in lies
            ]
            w = w[0] if len(w) == 1 else jnp.concatenate(w, axis=1)
            d = jnp.dot(returned[g], w, preferred_element_type=F32)
            total = d if total is None else total + d
        return total

    def returns(slot):
        source = (group + 4 - slot) % 4
        for part in (0, 1):
            two = pl.ds(part * 2 * HEAD, 2 * HEAD)
            arrival(returned.at[source, :, two], ret_recv.at[slot - 1, part])

    returns(2)
    for n, (lies, places) in enumerate(columns):
        if n == 2:
            twin_arrivals(far, cf_recv)
        total = project_out((group, (group + 2) % 4), lies)
        for begin, place in places:
            projected[:, place] = total[:, begin : begin + place.size]
    returns(1)
    returns(3)
    squares = jnp.zeros((ROWS, 1), F32)
    for lies, places in columns:
        total = project_out(((group + 3) % 4, (group + 1) % 4), lies)
        for begin, place in places:
            value = projected[:, place] + total[:, begin : begin + place.size]
            projected[:, place] = value
            squares = squares + jnp.sum(value * value, axis=-1, keepdims=True)
    scale = lax.rsqrt(squares * (1.0 / WIDTH) + EPS)
    written = []
    for n in range(4):
        rows = slice(n * (ROWS // 4), (n + 1) * (ROWS // 4))
        mixed[rows, :] = (projected[rows, :] * scale[rows] * out_gain[...]).astype(BF16)
        written.append(
            pltpu.make_async_copy(mixed.at[pl.ds(n * (ROWS // 4), ROWS // 4)], out.at[0, pl.ds(n * (ROWS // 4), ROWS // 4)], out_sem.at[n])
        )
        written[-1].start()

    ring_bytes, twin_bytes = pl.ds(0, Z - 1), pl.ds(0, Z)
    for buf, zs, _, cs, _ in (kv_ring, q_ring, near_ring):
        arrival(buf.at[ring_bytes], zs)
        arrival(buf.at[twin_bytes], cs)
    arrival(far.at[ring_bytes], far_send)
    arrival(far.at[twin_bytes], cf_send)
    arrival(raw, ag_send)
    arrival(kbuf.at[pl.ds(0, 3)], kv_send.at[0])
    arrival(vbuf.at[pl.ds(0, 3), pl.ds(0, HEAD)], kv_send.at[1])
    arrival(attended.at[pl.ds(0, 3)], ret_send)
    for copy in written:
        copy.wait()


def on_device(tokens, in_gain, wq, wk, wv, q_gain, k_gain, wo, out_gain):
    hbm = pl.BlockSpec(memory_space=pl.ANY)
    dma = pltpu.SemaphoreType.DMA
    one = dma(())
    ring = dma((2, 4, 2))
    return pl.pallas_call(
        kernel,
        out_shape=jax.ShapeDtypeStruct((1, ROWS, WIDTH), BF16),
        in_specs=[hbm] * 9,
        out_specs=hbm,
        scratch_shapes=[
            pltpu.VMEM((1, WIDTH), F32),
            pltpu.VMEM((1, HEAD), F32),
            pltpu.VMEM((1, HEAD), F32),
            pltpu.VMEM((1, WIDTH), F32),
            pltpu.VMEM((ROWS, WIDTH), BF16),
            pltpu.VMEM(wq.shape, BF16),
            pltpu.VMEM(wk.shape, BF16),
            pltpu.VMEM(wv.shape, BF16),
            pltpu.VMEM(wo.shape, BF16),
            pltpu.VMEM((3, ROWS, WIDTH), BF16),
            pltpu.VMEM((GROUP, ROWS, WIDTH), BF16),
            pltpu.VMEM((2 * Z, SHARD, 2 * HEAD), BF16),
            pltpu.VMEM((2 * Z, SHARD, 512), BF16),
            pltpu.VMEM((2 * Z, SHARD, NEAR), BF16),
            pltpu.VMEM((2 * Z, SHARD, FAR), BF16),
            pltpu.VMEM((GROUP, ROWS, HEAD), F32),
            pltpu.VMEM((GROUP, ROWS, HEAD), F32),
            pltpu.VMEM((GROUP, HEAD, ROWS), F32),
            pltpu.VMEM((GROUP, HEAD, ROWS), F32),
            pltpu.VMEM((2 * HEAD, KEYS * GROUP), BF16),
            pltpu.VMEM((GROUP, KEYS, HEAD), BF16),
            pltpu.VMEM((GROUP, HEAD + ONES, KEYS), BF16),
            pltpu.VMEM((KEYS, BQ), F32),
            pltpu.VMEM((KEYS, BQ), F32),
            pltpu.VMEM((8, BQ), F32),
            pltpu.VMEM((8, BQ), F32),
            pltpu.VMEM((1, KEYS * GROUP), F32),
            pltpu.VMEM((HEAD + ONES, KEYS * GROUP), F32),
            pltpu.VMEM((GROUP, ROWS, 512), BF16),
            pltpu.VMEM((GROUP, ROWS, 512), BF16),
            pltpu.VMEM((ROWS, WIDTH), F32),
            pltpu.VMEM((ROWS, WIDTH), BF16),
            dma((9,)),
            dma((4,)),
            one,
            dma((6,)),
            *([one, ring, one, one] * 3),
            one,
            dma((Z, 2)),
            one,
            one,
            dma((2,)),
            dma((12,)),
            one,
            dma((3, 2)),
        ],
        compiler_params=pltpu.CompilerParams(
            collective_id=0, has_side_effects=True, vmem_limit_bytes=60 * 2**20
        ),
        name="grouped_attention",
    )(
        tokens,
        in_gain.reshape(1, WIDTH),
        wq,
        wk,
        wv,
        q_gain.reshape(1, HEAD),
        k_gain.reshape(1, HEAD),
        wo,
        out_gain.reshape(1, WIDTH),
    )


def solution(mesh):
    placed = (
        P("dp", "sp", None),
        P(),
        P("dp", None),
        P("dp", None),
        P("dp", None),
        P(),
        P(),
        P("dp", None),
        P(),
    )
    return jax.shard_map(
        on_device, mesh=mesh, in_specs=placed, out_specs=P("dp", "sp", None), check_vma=False
    )
```
